256 devices in a mesh: sp: 64 (over z, y, core), tp: 4 (over x).
Axes of the slice: x: 4, y: 4, z: 8, core: 2. Of those that a mesh axis runs over, the one named last changes fastest.
Arguments:
- stream_in: bfloat16 [16384, 2048], P(('sp', 'tp')), may hold values from -6 to 6
- queries_one: bfloat16 [16384, 1024], P('sp', 'tp'), may hold values from -120 to 120
- queries_two: bfloat16 [16384, 1024], P('sp', 'tp'), may hold values from -120 to 120
- keys_one: bfloat16 [16384, 512], P('sp', 'tp'), may hold values from -7 to 7
- keys_two: bfloat16 [16384, 512], P('sp', 'tp'), may hold values from -7 to 7
- values: bfloat16 [16384, 1024], P('sp', 'tp'), may hold values from -6 to 6
- lambdas: float32 [8], P('tp'), may hold values from 0.3 to 0.8
- head_gain: float32 [256], replicated, may hold values from 0.1 to 1.9
- out_weight: bfloat16 [2048, 2048], P('tp'), may hold values from -0.125 to 0.125
- norm_gain: float32 [2048], replicated, may hold values from 0.1 to 1.9
- expert_ids: int32 [16384, 2], P(('sp', 'tp')), may hold values from 0 to 63, all different within a row; in each aligned block of 64 rows (0 to 63, 64 to 127, ...) at most 4 rows name the same one
- route_weight: float32 [16384, 2], P(('sp', 'tp')), may hold values from 0.1 to 1
- gate_weight: bfloat16 [64, 2048, 1024], P('sp', None, 'tp'), may hold values from -0.125 to 0.125
- up_weight: bfloat16 [64, 2048, 1024], P('sp', None, 'tp'), may hold values from -0.125 to 0.125
- down_weight: bfloat16 [64, 1024, 2048], P('sp', 'tp'), may hold values from -0.1875 to 0.1875
Outputs:
- mixed: bfloat16 [16384, 2048], P(('sp', 'tp'))
The draws below stay inside these ranges and needn't reach their ends.
Inputs may be any that keep to these rules, and one draw needn't show every extreme that they name: `expert_ids`: each row names 2 different experts. In each aligned block of 64 rows no expert is named more than 4 times, a bound that some block reaches.
All inputs are finite; a program needn't handle non-finite values.
Results may differ from the reference program's by a relative error of at most 0.013.
Values may be sent and summed in bfloat16 or wider, within the bound.
A program may use at most 128 MiB of HBM per device.

```python
import math
import jax
import jax.numpy as jnp
import numpy as np
from jax import lax

D = 2048
HEADS = 8
KV_HEADS = 4
HEAD_DIM = 128
VAL_DIM = 256
EXPERT_FF = 1024
TOPK = 2
TOKENS = 16384
ROWS_DEV = 64
EXPERTS = 64
CAP = 4
N_SP = 64
N_TP = 4


def attention_draw(key):
    keys_first = jnp.clip(jax.random.normal(jax.random.fold_in(key, 11), (TOKENS, KV_HEADS * HEAD_DIM), jnp.float32) * 1.2, -7.0, 7.0)
    keys_second = jnp.clip(jax.random.normal(jax.random.fold_in(key, 12), (TOKENS, KV_HEADS * HEAD_DIM), jnp.float32) * 1.2, -7.0, 7.0)
    query_first = jnp.clip(jax.random.normal(jax.random.fold_in(key, 13), (TOKENS, HEADS * HEAD_DIM), jnp.float32) * 1.5, -9.0, 9.0)
    query_second = jnp.clip(jax.random.normal(jax.random.fold_in(key, 14), (TOKENS, HEADS * HEAD_DIM), jnp.float32) * 1.5, -9.0, 9.0)
    return (query_first, query_second, keys_first, keys_second)


def draw_queries_one(key, part):
    return attention_draw(key)[0].astype(jnp.bfloat16)


def draw_queries_two(key, part):
    return attention_draw(key)[1].astype(jnp.bfloat16)


def draw_keys_one(key, part):
    return attention_draw(key)[2].astype(jnp.bfloat16)


def draw_keys_two(key, part):
    return attention_draw(key)[3].astype(jnp.bfloat16)


def steps_of(key, dims, pieces, low, top_value):
    def one(position, blocks):
        heights = jax.random.uniform(jax.random.fold_in(jax.random.fold_in(key, 6), position), (blocks,), jnp.float32, low / len(pieces), top_value / len(pieces))
        return jnp.repeat(jnp.exp(heights), dims[position] // blocks).reshape((-1,) + (1,) * (len(dims) - position - 1))

    gain = one(*pieces[0])
    for cut in pieces[1:]:
        gain = gain * one(*cut)
    return gain


def deal_out(stream_key, own, number, rows, number_of, top, limit, lean):
    ranking = jax.random.permutation(stream_key, number_of)
    crowded, ordinary = shares(number_of, rows * top, limit, lean, True), shares(number_of, rows * top, limit, lean, False)
    places = jnp.arange(number_of)

    def named(lengths, turn):
        used = int((lengths > 0).sum())
        fixed = max(1, used // 4)
        shifted = fixed + (places - fixed + turn * (used - fixed)) % max(1, number_of - fixed)
        return jnp.zeros((number_of,), jnp.int32).at[ranking[jnp.where(places < fixed, places, shifted)]].set(jnp.asarray(lengths, jnp.int32))

    lengths = jnp.where(number % 4 == 0, named(crowded, number // 4), named(ordinary, number - number // 4 - 1))
    mixed = jax.random.permutation(jax.random.fold_in(own, 3), number_of)
    giver, receiver = mixed[0:number_of // 2 * 2:2], mixed[1:number_of // 2 * 2:2]
    room = jnp.minimum(lengths[giver] - 1, limit - lengths[receiver]) // 2
    room = jnp.where((giver == ranking[0]) | (receiver == ranking[0]) | (lengths[receiver] == 0), 0, jnp.maximum(room, 0))
    shifted = jax.random.randint(jax.random.fold_in(own, 4), (number_of // 2,), 0, 1 << 20) % (room + 1)
    lengths = lengths.at[giver].add(-shifted).at[receiver].add(shifted)
    labels = jnp.searchsorted(jnp.cumsum(lengths), jnp.arange(rows * top), side="right").astype(jnp.int32)
    listing = labels.reshape(top, rows).T
    listing = listing[jax.random.permutation(jax.random.fold_in(own, 1), rows)]
    turn = jax.random.randint(jax.random.fold_in(own, 2), (rows, 1), 0, top)
    return jnp.take_along_axis(listing, (jnp.arange(top)[None, :] + turn) % top, axis=1)


def shares(count, total, limit, slope, full):
    loads = [(1 << 20) // math.isqrt(grade ** slope) + 1 for grade in range(1, count + 1)]
    largest = limit if full else min(limit, max(-(-total // count), total * loads[0] // sum(loads)))
    least = 1 if total - largest >= count - 1 else 0
    given, rest = [largest] + [least] * (count - 1), total - largest - least * (count - 1)
    while rest > 0:
        free = [i for i in range(1, count) if given[i] < largest] or [i for i in range(1, count) if given[i] < limit]
        whole, left = sum([loads[i] for i in free]), rest
        for i in free:
            more = min(limit - given[i], max(1, left * loads[i] // whole), rest)
            given[i] = given[i] + more
            rest = rest - more
    return np.array(given)


def gaussian(stream_key, extent, width, bound, split=(), kind=jnp.bfloat16):
    entries = jax.random.normal(stream_key, extent, jnp.float32) * width
    if len(split) > 0:
        entries = steps_of(stream_key, extent, split, -0.22, 0.18) * entries
    return jnp.clip(entries, min=-bound, max=bound).astype(kind)


def setup_inputs(seed: int = 0) -> dict:
    seeds = jax.random.split(jax.random.key(seed), 16)
    stream_in = gaussian(seeds[0], (TOKENS, D), 1.0, 6.0, ((0, 256),))
    queries_one = draw_queries_one(jax.random.fold_in(seeds[15], 71), 0)
    queries_two = draw_queries_two(jax.random.fold_in(seeds[15], 71), 0)
    keys_one = draw_keys_one(jax.random.fold_in(seeds[15], 71), 0)
    keys_two = draw_keys_two(jax.random.fold_in(seeds[15], 71), 0)
    values = gaussian(seeds[5], (TOKENS, KV_HEADS * VAL_DIM), 1.0, 6.0, ((0, 64), (1, 4)))
    lambdas = jnp.clip(0.3 + 0.5 * jax.random.uniform(seeds[6], (HEADS,), jnp.float32) ** steps_of(seeds[6], (HEADS,), ((0, 4),), -0.2, 0.2), 0.3, 0.8)
    head_gain = jnp.clip(1.0 + 0.18 * jax.random.normal(seeds[7], (VAL_DIM,), jnp.float32), 0.1, 1.9)
    out_weight = gaussian(seeds[8], (HEADS * VAL_DIM, D), (HEADS * VAL_DIM) ** -0.5, 0.125, ((0, 4),))
    norm_gain = jnp.clip(1.0 + 0.18 * jax.random.normal(seeds[9], (D,), jnp.float32), 0.1, 1.9)
    expert_ids_keys = jax.random.split(jax.random.fold_in(seeds[10], 1), TOKENS // ROWS_DEV)
    expert_ids_turns = jax.random.permutation(jax.random.fold_in(seeds[10], 3), TOKENS // ROWS_DEV)
    expert_ids = jax.vmap(lambda own, number: deal_out(jax.random.fold_in(seeds[10], 2), own, number, ROWS_DEV, EXPERTS, TOPK, CAP, 1))(expert_ids_keys, expert_ids_turns).reshape((TOKENS, TOPK))
    route_weight = jnp.clip(0.1 + 0.9 * jax.random.uniform(seeds[11], (TOKENS, TOPK), jnp.float32) ** steps_of(seeds[11], (TOKENS, TOPK), ((0, 256),), -0.2, 0.2), 0.1, 1.0)
    gate_weight = gaussian(seeds[12], (EXPERTS, D, EXPERT_FF), D ** -0.5, 0.125, ((0, 64), (2, 4)))
    up_weight = gaussian(seeds[13], (EXPERTS, D, EXPERT_FF), D ** -0.5, 0.125, ((0, 64), (2, 4)))
    down_weight = gaussian(seeds[14], (EXPERTS, EXPERT_FF, D), EXPERT_FF ** -0.5, 0.1875, ((0, 64), (1, 4)))
    return {"stream_in": stream_in, "queries_one": queries_one, "queries_two": queries_two, "keys_one": keys_one, "keys_two": keys_two, "values": values, "lambdas": lambdas, "head_gain": head_gain, "out_weight": out_weight, "norm_gain": norm_gain, "expert_ids": expert_ids, "route_weight": route_weight, "gate_weight": gate_weight, "up_weight": up_weight, "down_weight": down_weight}


EPS = 1e-06
OUT_SCALE = 0.8

def mix_map(queries, keys, vals, allowed):
    scores = jnp.einsum('qrd,kd->rqk', queries, keys) * HEAD_DIM ** (-0.5)
    scores = jnp.where(allowed[None], scores, -jnp.inf)
    row_max = lax.optimization_barrier(jnp.max(scores, axis=-1, keepdims=True))
    exp_terms = jnp.exp(scores - row_max)
    totals = lax.optimization_barrier(jnp.sum(exp_terms, axis=-1, keepdims=True))
    weights = lax.optimization_barrier(exp_terms.astype(jnp.bfloat16)).astype(jnp.float32)
    return jnp.einsum('rqk,kv->rqv', weights, vals) / totals

def reference(stream_in, queries_one, queries_two, keys_one, keys_two, values, lambdas, head_gain, out_weight, norm_gain, expert_ids, route_weight, gate_weight, up_weight, down_weight):
    per_kv = HEADS // KV_HEADS
    q_block = math.gcd(TOKENS, 512)
    num_blocks = TOKENS // q_block
    key_pos = jnp.arange(TOKENS, dtype=jnp.int32)
    keys_first = keys_one.astype(jnp.float32)
    keys_second = keys_two.astype(jnp.float32)
    vals_all = values.astype(jnp.float32)

    def one_block(block_index):
        first_row = (block_index * q_block).astype(jnp.int32)
        q_first = lax.dynamic_slice_in_dim(queries_one, first_row, q_block, 0).astype(jnp.float32).reshape(q_block, HEADS, HEAD_DIM)
        q_second = lax.dynamic_slice_in_dim(queries_two, first_row, q_block, 0).astype(jnp.float32).reshape(q_block, HEADS, HEAD_DIM)
        query_pos = first_row + jnp.arange(q_block, dtype=jnp.int32)
        allowed = key_pos[None, :] <= query_pos[:, None]
        head_outs = []
        for kv_index in range(KV_HEADS):
            lo_head = kv_index * per_kv
            key_cols = slice(kv_index * HEAD_DIM, (kv_index + 1) * HEAD_DIM)
            val_cols = slice(kv_index * VAL_DIM, (kv_index + 1) * VAL_DIM)
            mix_first = mix_map(q_first[:, lo_head:lo_head + per_kv], keys_first[:, key_cols], vals_all[:, val_cols], allowed)
            mix_second = mix_map(q_second[:, lo_head:lo_head + per_kv], keys_second[:, key_cols], vals_all[:, val_cols], allowed)
            lambda_rows = lambdas[lo_head:lo_head + per_kv][:, None, None]
            head_outs.append(mix_first - lambda_rows * mix_second)
        difference = jnp.concatenate(head_outs, 0)
        mean_sq = lax.optimization_barrier(jnp.mean(difference * difference, axis=-1, keepdims=True))
        normed_heads = difference * lax.rsqrt(mean_sq + EPS) * head_gain * OUT_SCALE
        return normed_heads.transpose(1, 0, 2).reshape(q_block, HEADS * VAL_DIM).astype(jnp.bfloat16)
    heads_out = lax.map(one_block, jnp.arange(num_blocks, dtype=jnp.int32)).reshape(TOKENS, HEADS * VAL_DIM)
    col_width = HEADS * VAL_DIM // N_TP
    stream = stream_in.astype(jnp.float32)
    for group_no in range(N_TP):
        cols = slice(group_no * col_width, (group_no + 1) * col_width)
        partial_value = jnp.dot(heads_out[:, cols], out_weight[cols], preferred_element_type=jnp.float32)
        stream = stream + lax.optimization_barrier(partial_value.astype(jnp.bfloat16)).astype(jnp.float32)
    normed = (stream * lax.rsqrt(lax.optimization_barrier(jnp.mean(stream * stream, axis=-1, keepdims=True)) + EPS) * norm_gain).astype(jnp.bfloat16)
    flat_ids = expert_ids.reshape(-1)
    owners = jnp.arange(TOKENS * TOPK, dtype=jnp.int32) // TOPK
    rows_all = jnp.take(normed, owners, axis=0)
    capacity = N_SP * N_TP * CAP
    quarter = EXPERT_FF // N_TP

    def per_expert(collected, weights_item):
        gate_w, up_w, down_w, number = weights_item
        chosen = flat_ids == number
        places = jnp.cumsum(chosen.astype(jnp.int32)) - 1
        target = jnp.where(chosen, places, capacity).astype(jnp.int32)
        buffer = jnp.zeros((capacity + 1, D), jnp.bfloat16).at[target].set(rows_all)[:capacity]
        gate = jnp.dot(buffer, gate_w, preferred_element_type=jnp.float32)
        upper = jnp.dot(buffer, up_w, preferred_element_type=jnp.float32)
        hidden = (jax.nn.silu(gate) * upper).astype(jnp.bfloat16)
        summed = jnp.zeros((capacity, D), jnp.float32)
        for group_no in range(N_TP):
            units = slice(group_no * quarter, (group_no + 1) * quarter)
            partial_value = jnp.dot(hidden[:, units], down_w[units], preferred_element_type=jnp.float32)
            summed = summed + lax.optimization_barrier(partial_value.astype(jnp.bfloat16)).astype(jnp.float32)
        result = jnp.concatenate([summed.astype(jnp.bfloat16), jnp.zeros((1, D), jnp.bfloat16)], 0)
        collected = jnp.where(chosen[:, None], jnp.take(result, target, axis=0), collected)
        return (collected, None)
    collected, _ = lax.scan(per_expert, jnp.zeros((TOKENS * TOPK, D), jnp.bfloat16), (gate_weight, up_weight, down_weight, jnp.arange(EXPERTS, dtype=jnp.int32)))
    routed = lax.optimization_barrier(jnp.sum(collected.reshape(TOKENS, TOPK, D).astype(jnp.float32) * route_weight[:, :, None], axis=1))
    return (stream + routed).astype(jnp.bfloat16)
```

```python
import functools
import math

import jax
import jax.numpy as jnp
from jax import lax
from jax.experimental import pallas as pl
from jax.experimental.pallas import tpu as pltpu
from jax.sharding import PartitionSpec as P

HEAD_DIM = 128
VAL_DIM = 256
EPS = 1e-06
OUT_SCALE = 0.8
SCALE2 = HEAD_DIM ** (-0.5) * math.log2(math.e)
BK = 1024


def flash_kernel(n_sp, q_ref, kv_ref, lam_ref, gain_ref, out_ref, m_ref, l_ref, acc_ref):
    me = lax.axis_index("sp")
    rows = q_ref.shape[2]
    half = rows // 2

    def update(run, block, masked, first_row):
        start = pl.multiple_of(block * BK, BK)
        v = kv_ref[pl.ds(start, BK), 2 * HEAD_DIM :]
        if masked:
            row = first_row + lax.rem(lax.broadcasted_iota(jnp.int32, (rows, BK), 0), half)
            keep = start + lax.broadcasted_iota(jnp.int32, (rows, BK), 1) <= row
        for k in range(2):
            q = q_ref[run, k]
            keys = kv_ref[pl.ds(start, BK), k * HEAD_DIM : (k + 1) * HEAD_DIM]
            s = lax.dot_general(q, keys, (((1,), (1,)), ((), ())), preferred_element_type=jnp.float32)
            if masked:
                s = jnp.where(keep, s, -jnp.inf)
            old = m_ref[k]
            new = jnp.maximum(old, jnp.max(s, axis=1, keepdims=True))
            terms = jnp.exp2((s - new[:, :1]) * SCALE2)
            fade = jnp.exp2((old - new) * SCALE2)
            part = terms[:, :128]
            for c in range(1, BK // 128):
                part = part + terms[:, c * 128 : (c + 1) * 128]
            m_ref[k] = new
            l_ref[k] = l_ref[k] * fade + part
            acc_ref[k] = acc_ref[k] * fade[:, :1] + jnp.dot(
                terms.astype(jnp.bfloat16), v, preferred_element_type=jnp.float32
            )

    for run in range(2):
        first_row = me * 2 * half if run == 0 else (n_sp - 1 - me) * 2 * half + half
        m_ref[...] = jnp.full(m_ref.shape, -1e30, jnp.float32)
        l_ref[...] = jnp.zeros(l_ref.shape, jnp.float32)
        acc_ref[...] = jnp.zeros(acc_ref.shape, jnp.float32)
        full = first_row // BK
        lax.fori_loop(0, full, lambda i, c: (update(run, i, False, first_row), c)[1], 0)
        update(run, full, True, first_row)
        mix = [acc_ref[k] / jnp.sum(l_ref[k], axis=1, keepdims=True) for k in range(2)]
        for h in range(2):
            piece = slice(h * half, (h + 1) * half)
            diff = mix[0][piece] - lam_ref[h] * mix[1][piece]
            ms = jnp.mean(diff * diff, axis=1, keepdims=True)
            res = diff * lax.rsqrt(ms + EPS) * gain_ref[...] * OUT_SCALE
            out_ref[run * half : (run + 1) * half, h * VAL_DIM : (h + 1) * VAL_DIM] = res.astype(jnp.bfloat16)


def flash(q, kv, lambdas, gain, n_sp):
    rows = q.shape[2]
    return pl.pallas_call(
        functools.partial(flash_kernel, n_sp),
        out_shape=jax.ShapeDtypeStruct((rows, 2 * VAL_DIM), jnp.bfloat16),
        in_specs=[
            pl.BlockSpec(memory_space=pltpu.VMEM),
            pl.BlockSpec(memory_space=pltpu.VMEM),
            pl.BlockSpec(memory_space=pltpu.SMEM),
            pl.BlockSpec(memory_space=pltpu.VMEM),
        ],
        out_specs=pl.BlockSpec(memory_space=pltpu.VMEM),
        scratch_shapes=[
            pltpu.VMEM((2, rows, 128), jnp.float32),
            pltpu.VMEM((2, rows, 128), jnp.float32),
            pltpu.VMEM((2, rows, VAL_DIM), jnp.float32),
        ],
        compiler_params=pltpu.CompilerParams(vmem_limit_bytes=48 * 1024 * 1024),
        name="flash",
    )(q, kv, lambdas, gain)


def shards(
    stream_in, queries_one, queries_two, keys_one, keys_two, values, lambdas, head_gain, out_weight,
    norm_gain, expert_ids, route_weight, gate_weight, up_weight, down_weight,
):
    n_sp, n_tp = lax.axis_size("sp"), lax.axis_size("tp")
    rows = queries_one.shape[0]
    half = rows // 2
    feats = stream_in.shape[1] // n_tp
    bf, f32 = jnp.bfloat16, jnp.float32

    mirror = [(s, n_sp - 1 - s) for s in range(n_sp)]
    home = [
        (s * n_tp + t, (s if t < n_tp // 2 else n_sp - 1 - s) * n_tp + t)
        for s in range(n_sp)
        for t in range(n_tp)
    ]
    q_pair = jnp.stack([queries_one, queries_two])
    q_far = lax.ppermute(q_pair[:, half:], "sp", mirror)
    q_all = jnp.stack([q_pair[:, :half], q_far])
    q_all = q_all.reshape(2, 2, half, 2, HEAD_DIM).transpose(0, 1, 3, 2, 4).reshape(2, 2, rows, HEAD_DIM)
    stream_far = lax.ppermute(stream_in, ("sp", "tp"), home)
    stream_mine = lax.all_to_all(stream_far, "tp", 1, 0, tiled=True).astype(f32)
    ids = lax.all_gather(lax.ppermute(expert_ids, ("sp", "tp"), home), "tp", axis=0, tiled=True)
    route = lax.all_gather(lax.ppermute(route_weight, ("sp", "tp"), home), "tp", axis=0, tiled=True)
    out_cols = lax.all_to_all(out_weight, "tp", 1, 0, tiled=True)
    down_cols = lax.all_to_all(down_weight[0], "tp", 1, 0, tiled=True)
    gain_mine = lax.dynamic_slice_in_dim(norm_gain, lax.axis_index("tp") * feats, feats, 0)

    cap = 16
    flat = ids.reshape(-1)
    one_hot = (flat[:, None] == lax.iota(jnp.int32, n_sp)[None, :]).astype(bf)
    lower = (lax.iota(jnp.int32, 2 * rows)[:, None] > lax.iota(jnp.int32, 2 * rows)[None, :]).astype(bf)
    before = jnp.dot(lower, one_hot, preferred_element_type=f32)
    ranks = jnp.sum(before * one_hot.astype(f32), axis=1).astype(jnp.int32)
    slots = (flat * cap + ranks).reshape(rows, 2)
    pick = [(slots[:, k][:, None] == lax.iota(jnp.int32, n_sp * cap)[None, :]).astype(bf) for k in range(2)]

    packed = jnp.concatenate([keys_one, keys_two, values], 1)
    kv = lax.all_gather(packed, "sp", axis=0, tiled=True)
    heads = flash(q_all, kv, lambdas, head_gain[None], n_sp)
    heads_all = lax.all_gather(heads, "tp", axis=1, tiled=True)
    stream = stream_mine + jnp.dot(heads_all, out_cols, preferred_element_type=f32)
    ssq = lax.psum(jnp.sum(stream * stream, axis=1), "tp")
    inv = lax.rsqrt(ssq / (feats * n_tp) + EPS)
    normed = (stream * inv[:, None] * gain_mine).astype(bf)
    send = lax.dot_general(
        pick[0] + pick[1], normed, (((0,), (0,)), ((), ())), preferred_element_type=f32
    ).astype(bf)
    got = lax.all_to_all(send, "sp", 0, 0, tiled=True)
    got = lax.all_gather(got, "tp", axis=1, tiled=True)
    gate = jnp.dot(got, gate_weight[0], preferred_element_type=f32)
    upper = jnp.dot(got, up_weight[0], preferred_element_type=f32)
    hidden = (jax.nn.silu(gate) * upper).astype(bf)
    hidden = lax.all_gather(hidden, "tp", axis=1, tiled=True)
    result = jnp.dot(hidden, down_cols, preferred_element_type=f32).astype(bf)
    back = lax.all_to_all(result, "sp", 0, 0, tiled=True)
    for k in range(2):
        stream = stream + route[:, k][:, None] * jnp.dot(pick[k], back, preferred_element_type=f32)
    mixed = lax.all_to_all(stream.astype(bf), "tp", 0, 1, tiled=True)
    return lax.ppermute(mixed, ("sp", "tp"), home)


def solution(mesh):
    return jax.shard_map(
        shards,
        mesh=mesh,
        in_specs=(
            P(("sp", "tp"), None),
            P("sp", "tp"),
            P("sp", "tp"),
            P("sp", "tp"),
            P("sp", "tp"),
            P("sp", "tp"),
            P("tp"),
            P(),
            P("tp", None),
            P(),
            P(("sp", "tp"), None),
            P(("sp", "tp"), None),
            P("sp", None, "tp"),
            P("sp", None, "tp"),
            P("sp", "tp", None),
        ),
        out_specs=P(("sp", "tp"), None),
        check_vma=False,
    )
```

```python
import functools
import math

import jax
import jax.numpy as jnp
from jax import lax
from jax.experimental import pallas as pl
from jax.experimental.pallas import tpu as pltpu
from jax.sharding import PartitionSpec as P

HEAD_DIM = 128
VAL_DIM = 256
EPS = 1e-06
OUT_SCALE = 0.8
SCALE2 = HEAD_DIM ** (-0.5) * math.log2(math.e)
BK = 1024
PLANES = 8


def flash_kernel(n_sp, q_ref, kv_ref, lam_ref, gain_ref, out_ref, m_ref, l_ref, acc_ref):
    me = lax.axis_index("sp")
    rows = q_ref.shape[2]
    half = rows // 2

    def update(run, block, masked, first_row):
        start = pl.multiple_of(block * BK, BK)
        v = kv_ref[pl.ds(start, BK), 2 * HEAD_DIM :]
        if masked:
            row = first_row + lax.rem(lax.broadcasted_iota(jnp.int32, (rows, BK), 0), half)
            keep = start + lax.broadcasted_iota(jnp.int32, (rows, BK), 1) <= row
        for k in range(2):
            q = q_ref[run, k]
            keys = kv_ref[pl.ds(start, BK), k * HEAD_DIM : (k + 1) * HEAD_DIM]
            s = lax.dot_general(q, keys, (((1,), (1,)), ((), ())), preferred_element_type=jnp.float32)
            if masked:
                s = jnp.where(keep, s, -jnp.inf)
            old = m_ref[k]
            new = jnp.maximum(old, jnp.max(s, axis=1, keepdims=True))
            terms = jnp.exp2((s - new[:, :1]) * SCALE2)
            fade = jnp.exp2((old - new) * SCALE2)
            part = terms[:, :128]
            for c in range(1, BK // 128):
                part = part + terms[:, c * 128 : (c + 1) * 128]
            m_ref[k] = new
            l_ref[k] = l_ref[k] * fade + part
            acc_ref[k] = acc_ref[k] * fade[:, :1] + jnp.dot(
                terms.astype(jnp.bfloat16), v, preferred_element_type=jnp.float32
            )

    for run in range(2):
        first_row = me * 2 * half if run == 0 else (n_sp - 1 - me) * 2 * half + half
        m_ref[...] = jnp.full(m_ref.shape, -1e30, jnp.float32)
        l_ref[...] = jnp.zeros(l_ref.shape, jnp.float32)
        acc_ref[...] = jnp.zeros(acc_ref.shape, jnp.float32)
        full = first_row // BK
        lax.fori_loop(0, full, lambda i, c: (update(run, i, False, first_row), c)[1], 0)
        update(run, full, True, first_row)
        mix = [acc_ref[k] / jnp.sum(l_ref[k], axis=1, keepdims=True) for k in range(2)]
        for h in range(2):
            piece = slice(h * half, (h + 1) * half)
            diff = mix[0][piece] - lam_ref[h] * mix[1][piece]
            ms = jnp.mean(diff * diff, axis=1, keepdims=True)
            res = diff * lax.rsqrt(ms + EPS) * gain_ref[...] * OUT_SCALE
            out_ref[run * half : (run + 1) * half, h * VAL_DIM : (h + 1) * VAL_DIM] = res.astype(jnp.bfloat16)


def flash(q, kv, lambdas, gain, n_sp):
    rows = q.shape[2]
    return pl.pallas_call(
        functools.partial(flash_kernel, n_sp),
        out_shape=jax.ShapeDtypeStruct((rows, 2 * VAL_DIM), jnp.bfloat16),
        in_specs=[
            pl.BlockSpec(memory_space=pltpu.VMEM),
            pl.BlockSpec(memory_space=pltpu.VMEM),
            pl.BlockSpec(memory_space=pltpu.SMEM),
            pl.BlockSpec(memory_space=pltpu.VMEM),
        ],
        out_specs=pl.BlockSpec(memory_space=pltpu.VMEM),
        scratch_shapes=[
            pltpu.VMEM((2, rows, 128), jnp.float32),
            pltpu.VMEM((2, rows, 128), jnp.float32),
            pltpu.VMEM((2, rows, VAL_DIM), jnp.float32),
        ],
        compiler_params=pltpu.CompilerParams(vmem_limit_bytes=48 * 1024 * 1024),
        name="flash",
    )(q, kv, lambdas, gain)


MESH = pl.DeviceIdType.MESH


def post_kernel(n_sp, n_tp, group, heads, out_w, stream_in, gain, slots_row, slots_col, route, gate_h, up_h, down_h,
                out, hall, oc, gate_w, up_w, down_w, stream, ssq, send, xbuf, hbuf, rbuf, back, mix,
                sent, local_sem, wsem, asem, a2sem, qsem, dsem, xsem, x2sem, hsem, h2sem, bsem, fsem):
    s, t = lax.axis_index("sp"), lax.axis_index("tp")
    n_z = n_sp // group
    z, w = s // group, lax.rem(s, group)
    far_s = n_sp - 1 - s
    cap, feats = send.shape[1], send.shape[2]
    units = gate_w.shape[1]
    rows = heads.shape[0]
    half, block = rows // 2, rows // n_tp
    f32, bf = jnp.float32, jnp.bfloat16

    loads = [
        pltpu.make_async_copy(a, b, wsem.at[i])
        for i, (a, b) in enumerate(((out_w, oc), (gate_h, gate_w), (up_h, up_w), (down_h, down_w)))
    ]
    for load in loads:
        load.start()

    def side(d):
        return lax.rem(t + d + n_tp, n_tp)

    def offset(j):
        away = (n_z // 2 - j // 2) * jnp.minimum(j, 1)
        return away * (1 - 2 * lax.rem(j, 2))

    def to_plane(j):
        return lax.rem(z + offset(j) + n_z, n_z)

    def from_plane(j):
        return lax.rem(z - offset(j) + n_z, n_z)

    def remote(src, dst, a, b, sp, tp):
        return pltpu.make_async_remote_copy(
            src_ref=src, dst_ref=dst, send_sem=a, recv_sem=b, device_id=(sp, tp), device_id_type=MESH)

    def arrived(ref, sem):
        remote(ref, ref, sent.at[0], sem, s, side(1)).wait_recv()

    def left(ref, sem):
        remote(ref, ref, sem, dsem.at[0], s, side(1)).wait_send()

    barrier = pltpu.get_barrier_semaphore()

    def hello(sp, tp):
        pl.semaphore_signal(barrier, inc=1, device_id=(sp, tp), device_id_type=MESH)

    def greet(o, c):
        hello(lax.rem(s + o, n_sp), t)
        return c

    lax.fori_loop(1, n_sp, greet, 0)
    for d in range(1, n_tp):
        hello(s, side(d))
    low = t < n_tp // 2

    @pl.when(jnp.logical_not(low))
    def _():
        for d in range(n_tp):
            hello(far_s, d)

    pl.semaphore_wait(barrier, n_sp - 1 + n_tp - 1 + n_tp // 2)

    for k, d in enumerate((1, -1)):
        remote(heads, hall.at[t], sent.at[6], asem.at[k], s, side(d)).start()
    loads[0].wait()

    width = heads.shape[1]

    def project(x, q):
        return jnp.dot(x, oc[pl.ds(pl.multiple_of(q * width, width), width)], preferred_element_type=f32)

    stream[...] = stream_in[...].astype(f32) + project(heads[...], t)
    for k, d in enumerate((-1, 1)):
        arrived(hall.at[side(d)], asem.at[k])
        ref = hall.at[side(d), pl.ds(k * half, half)]
        remote(ref, ref, sent.at[7], a2sem.at[k], s, side(-d)).start()
    stream[...] += project(hall[side(-1)], side(-1)) + project(hall[side(1)], side(1))
    for k in range(2):
        arrived(hall.at[side(2), pl.ds(k * half, half)], a2sem.at[k])
    total = stream[...] + project(hall[side(2)], side(2))
    stream[...] = total

    part = jnp.sum(total * total, axis=1, keepdims=True)
    ssq[t] = jnp.broadcast_to(part, (rows, 128)).T[:8]
    for d in range(1, n_tp):
        remote(ssq.at[t], ssq.at[t], sent.at[8], qsem.at[d], s, side(d)).start()
    for d in range(1, n_tp):
        arrived(ssq.at[side(-d)], qsem.at[d])
    sums = ssq[0]
    for q in range(1, n_tp):
        sums = sums + ssq[q]
    inv = lax.rsqrt(sums / (feats * n_tp) + EPS)
    inv = jnp.concatenate([inv] * 16, axis=0).T[:, :1]
    normed = (stream[...] * inv * gain[...]).astype(bf)

    own = pltpu.make_async_copy(send.at[s], xbuf.at[t, s], local_sem.at[0])

    def pack(j):
        plane = to_plane(j)
        place = plane * (group * cap) + lax.broadcasted_iota(jnp.int32, (group * cap, rows), 0)
        chosen = (place == slots_row[0:1]) | (place == slots_row[1:2])
        picked = jnp.dot(jnp.where(chosen, 1.0, 0.0).astype(bf), normed, preferred_element_type=f32)
        send[pl.ds(pl.multiple_of(plane * group, group), group)] = picked.astype(bf).reshape(group, cap, feats)
        return plane

    pack(0)
    own.start()

    def near(i, c):
        dest = z * group + lax.rem(w + i, group)
        remote(send.at[dest], xbuf.at[t, s], sent.at[0], dsem.at[0], dest, t).start()
        return c

    lax.fori_loop(1, group, near, 0)

    def far(j, c):
        plane = pack(j)

        def one(i, c):
            dest = plane * group + lax.rem(w + i, group)
            remote(send.at[dest], xbuf.at[t, s], sent.at[0], dsem.at[j], dest, t).start()
            return c

        return lax.fori_loop(0, group, one, c)

    lax.fori_loop(1, n_z, far, 0)
    for load in loads[1:]:
        load.wait()

    def chunk(q, j):
        return xbuf.at[q, pl.ds(from_plane(j) * group, group)]

    def stage_x(j):
        @pl.when(j == 0)
        def _():
            own.wait()
            arrived(xbuf.at[t, pl.ds(0, group - 1)], dsem.at[0])

        @pl.when(j > 0)
        def _():
            arrived(chunk(t, j), dsem.at[j])

        for k, d in enumerate((1, -1)):
            remote(chunk(t, j), chunk(t, j), sent.at[1], xsem.at[k, j], s, side(d)).start()

    def stage_x2(j):
        arrived(chunk(side(-1), j), xsem.at[0, j])
        arrived(chunk(side(1), j), xsem.at[1, j])
        d = 1 - 2 * lax.rem(j, 2)
        ref = chunk(side(-d), j)
        remote(ref, ref, sent.at[2], x2sem.at[j], s, side(d)).start()

    def stage_up(j):
        arrived(chunk(side(2), j), x2sem.at[j])
        first = pl.multiple_of(from_plane(j) * group, group)
        gate = jnp.zeros((group * cap, units), f32)
        upper = jnp.zeros((group * cap, units), f32)
        for q in range(n_tp):
            x = xbuf[q, pl.ds(first, group)].reshape(group * cap, feats)
            gate = gate + jnp.dot(x, gate_w[q * feats : (q + 1) * feats], preferred_element_type=f32)
            upper = upper + jnp.dot(x, up_w[q * feats : (q + 1) * feats], preferred_element_type=f32)
        act = gate / (1.0 + jnp.exp(-gate)) * upper
        plane = from_plane(j)
        hbuf[t, plane] = act.astype(bf)
        for k, d in enumerate((1, -1)):
            ref = hbuf.at[t, plane]
            remote(ref, ref, sent.at[3], hsem.at[k, j], s, side(d)).start()

    def stage_h2(j):
        plane = from_plane(j)
        arrived(hbuf.at[side(-1), plane], hsem.at[0, j])
        arrived(hbuf.at[side(1), plane], hsem.at[1, j])
        d = 1 - 2 * lax.rem(j, 2)
        ref = hbuf.at[side(-d), plane]
        remote(ref, ref, sent.at[4], h2sem.at[j], s, side(d)).start()

    def stage_down(j):
        plane = from_plane(j)
        arrived(hbuf.at[side(2), plane], h2sem.at[j])
        res = jnp.zeros((group * cap, feats), f32)
        for q in range(n_tp):
            res = res + jnp.dot(hbuf[q, plane], down_w[q * units : (q + 1) * units], preferred_element_type=f32)
        first = pl.multiple_of(plane * group, group)
        rbuf[pl.ds(first, group)] = res.astype(bf).reshape(group, cap, feats)

        @pl.when(j == 0)
        def _():
            pltpu.make_async_copy(rbuf.at[s], back.at[s], local_sem.at[1]).start()

            def one(i, c):
                dest = z * group + lax.rem(w + i, group)
                remote(rbuf.at[dest], back.at[s], sent.at[5], bsem.at[0], dest, t).start()
                return c

            lax.fori_loop(1, group, one, 0)

        @pl.when(j > 0)
        def _():
            def one(i, c):
                dest = plane * group + lax.rem(w + i, group)
                remote(rbuf.at[dest], back.at[s], sent.at[5], bsem.at[j], dest, t).start()
                return c

            lax.fori_loop(0, group, one, 0)

    stages = (stage_x, stage_x2, stage_up, stage_h2, stage_down)

    def step(i, c):
        for lag, stage in enumerate(stages):
            j = i - lag

            @pl.when((j >= 0) & (j < n_z))
            def _():
                stage(j)

        return c

    lax.fori_loop(0, n_z + len(stages) - 1, step, 0)

    pltpu.make_async_copy(rbuf.at[s], back.at[s], local_sem.at[1]).wait()
    arrived(back.at[pl.ds(0, group - 1)], bsem.at[0])

    def home(j, c):
        arrived(back.at[pl.ds(to_plane(j) * group, group)], bsem.at[j])
        return c

    lax.fori_loop(1, n_z, home, 0)

    table = back[...].reshape(n_sp * cap, feats)
    total = stream[...]
    place = lax.broadcasted_iota(jnp.int32, (rows, n_sp * cap), 1)
    for k in range(2):
        chosen = jnp.where(place == slots_col[:, k : k + 1], 1.0, 0.0).astype(bf)
        total = total + route[:, k : k + 1] * jnp.dot(chosen, table, preferred_element_type=f32)
    mix[...] = total.astype(bf)
    columns = out.at[:, pl.ds(pl.multiple_of(t * feats, feats), feats)]
    for b in range(n_tp):
        piece = mix.at[pl.ds(b * block, block)]
        if b < n_tp // 2:

            @pl.when(t == b)
            def _():
                pltpu.make_async_copy(piece, columns, local_sem.at[2]).start()

            @pl.when(t != b)
            def _():
                remote(piece, columns, sent.at[9], fsem.at[t], s, b).start()
        else:
            remote(piece, columns, sent.at[9], fsem.at[t], far_s, b).start()
    for q in range(n_tp):
        ref = out.at[:, pl.ds(q * feats, feats)]
        mine = (t == q) & low

        @pl.when(mine)
        def _():
            pltpu.make_async_copy(mix.at[pl.ds(0, block)], ref, local_sem.at[2]).wait()

        @pl.when(jnp.logical_not(mine))
        def _():
            arrived(ref, fsem.at[q])

    left(send.at[pl.ds(0, n_sp - 1)], sent.at[0])
    left(xbuf.at[pl.ds(0, 2)], sent.at[1])
    left(xbuf.at[0], sent.at[2])
    left(hbuf.at[pl.ds(0, 2)], sent.at[3])
    left(hbuf.at[0], sent.at[4])
    left(rbuf.at[pl.ds(0, n_sp - 1)], sent.at[5])
    left(hall.at[pl.ds(0, 2)], sent.at[6])
    left(hall.at[0], sent.at[7])
    left(ssq.at[pl.ds(0, n_tp - 1)], sent.at[8])

    @pl.when(low)
    def _():
        left(mix.at[pl.ds(0, (n_tp - 1) * block)], sent.at[9])

    @pl.when(jnp.logical_not(low))
    def _():
        left(mix, sent.at[9])


def post(heads, out_w, stream_in, gain, slots_row, slots_col, route, gate_w, up_w, down_w, n_sp, n_tp, group, cap):
    rows, feats = stream_in.shape
    units = gate_w.shape[1]
    n_z = n_sp // group
    bf, f32 = jnp.bfloat16, jnp.float32
    dma = pltpu.SemaphoreType.DMA
    vmem, hbm = pl.BlockSpec(memory_space=pltpu.VMEM), pl.BlockSpec(memory_space=pl.ANY)
    return pl.pallas_call(
        functools.partial(post_kernel, n_sp, n_tp, group),
        out_shape=jax.ShapeDtypeStruct((rows // n_tp, feats * n_tp), bf),
        in_specs=[vmem, hbm, vmem, vmem, vmem, vmem, vmem, hbm, hbm, hbm],
        out_specs=vmem,
        scratch_shapes=[
            pltpu.VMEM((n_tp,) + heads.shape, bf),
            pltpu.VMEM(out_w.shape, bf),
            pltpu.VMEM(gate_w.shape, bf),
            pltpu.VMEM(up_w.shape, bf),
            pltpu.VMEM(down_w.shape, bf),
            pltpu.VMEM((rows, feats), f32),
            pltpu.VMEM((n_tp, 8, rows), f32),
            pltpu.VMEM((n_sp, cap, feats), bf),
            pltpu.VMEM((n_tp, n_sp, cap, feats), bf),
            pltpu.VMEM((n_tp, n_z, group * cap, units), bf),
            pltpu.VMEM((n_sp, cap, feats), bf),
            pltpu.VMEM((n_sp, cap, feats), bf),
            pltpu.VMEM((rows, feats), bf),
            dma((10,)), dma((3,)), dma((4,)), dma((2,)), dma((2,)), dma((n_tp,)), dma((n_z,)), dma((2, n_z)),
            dma((n_z,)), dma((2, n_z)), dma((n_z,)), dma((n_z,)), dma((n_tp,)),
        ],
        compiler_params=pltpu.CompilerParams(
            collective_id=1, has_side_effects=True, vmem_limit_bytes=40 * 1024 * 1024),
        name="post",
    )(heads, out_w, stream_in, gain, slots_row, slots_col, route, gate_w, up_w, down_w)


def shards(
    stream_in, queries_one, queries_two, keys_one, keys_two, values, lambdas, head_gain, out_weight,
    norm_gain, expert_ids, route_weight, gate_weight, up_weight, down_weight,
):
    n_sp, n_tp = lax.axis_size("sp"), lax.axis_size("tp")
    rows = queries_one.shape[0]
    half = rows // 2
    feats = stream_in.shape[1] // n_tp
    bf, f32 = jnp.bfloat16, jnp.float32

    mirror = [(s, n_sp - 1 - s) for s in range(n_sp)]
    home = [
        (s * n_tp + t, (s if t < n_tp // 2 else n_sp - 1 - s) * n_tp + t)
        for s in range(n_sp)
        for t in range(n_tp)
    ]
    q_pair = jnp.stack([queries_one, queries_two])
    q_far = lax.ppermute(q_pair[:, half:], "sp", mirror)
    q_all = jnp.stack([q_pair[:, :half], q_far])
    q_all = q_all.reshape(2, 2, half, 2, HEAD_DIM).transpose(0, 1, 3, 2, 4).reshape(2, 2, rows, HEAD_DIM)
    stream_far = lax.ppermute(stream_in, ("sp", "tp"), home)
    stream_mine = lax.all_to_all(stream_far, "tp", 1, 0, tiled=True)
    ids = lax.all_gather(lax.ppermute(expert_ids, ("sp", "tp"), home), "tp", axis=0, tiled=True)
    route = lax.all_gather(lax.ppermute(route_weight, ("sp", "tp"), home), "tp", axis=0, tiled=True)
    out_cols = lax.all_to_all(out_weight, "tp", 1, 0, tiled=True)
    down_cols = lax.all_to_all(down_weight[0], "tp", 1, 0, tiled=True)
    gain_mine = lax.dynamic_slice_in_dim(norm_gain, lax.axis_index("tp") * feats, feats, 0)

    cap = 16
    flat = ids.reshape(-1)
    one_hot = (flat[:, None] == lax.iota(jnp.int32, n_sp)[None, :]).astype(bf)
    lower = (lax.iota(jnp.int32, 2 * rows)[:, None] > lax.iota(jnp.int32, 2 * rows)[None, :]).astype(bf)
    before = jnp.dot(lower, one_hot, preferred_element_type=f32)
    ranks = jnp.sum(before * one_hot.astype(f32), axis=1).astype(jnp.int32)
    slots = (flat * cap + ranks).reshape(rows, 2)
    packed = jnp.concatenate([keys_one, keys_two, values], 1)
    kv = lax.all_gather(packed, "sp", axis=0, tiled=True)
    heads = flash(q_all, kv, lambdas, head_gain[None], n_sp)
    return post(
        heads, out_cols, stream_mine, gain_mine[None], slots.T, slots, route, gate_weight[0], up_weight[0], down_cols,
        n_sp, n_tp, n_sp // PLANES, cap,
    )


def solution(mesh):
    return jax.shard_map(
        shards,
        mesh=mesh,
        in_specs=(
            P(("sp", "tp"), None),
            P("sp", "tp"),
            P("sp", "tp"),
            P("sp", "tp"),
            P("sp", "tp"),
            P("sp", "tp"),
            P("tp"),
            P(),
            P("tp", None),
            P(),
            P(("sp", "tp"), None),
            P(("sp", "tp"), None),
            P("sp", None, "tp"),
            P("sp", None, "tp"),
            P("sp", "tp", None),
        ),
        out_specs=P(("sp", "tp"), None),
        check_vma=False,
    )
```

```python
import functools
import math

import jax
import jax.numpy as jnp
from jax import lax
from jax.experimental import pallas as pl
from jax.experimental.pallas import tpu as pltpu
from jax.sharding import PartitionSpec as P

HEAD_DIM = 128
VAL_DIM = 256
EPS = 1e-06
OUT_SCALE = 0.8
SCALE2 = HEAD_DIM ** (-0.5) * math.log2(math.e)
MESH = pl.DeviceIdType.MESH
CHIPS = (8, 4, 2)
SPLIT = 144
CAP = 16


def front_kernel(dims, queries_one, queries_two, keys_one, keys_two, values, stream_in, meta_in, out_w, down_w, lam, gain,
                 heads, stream, meta, out_cols, down_cols, kv, q_far, q_all, m_ref, l_ref, acc_ref,
                 sent, local_sem, qsem, ssem, msem, osem, wsem, pz, py, py2, ry, ry2, rz, sib):
    n_z, n_y, n_c, n_tp, split = dims
    n_sp = n_z * n_y * n_c
    s, t = lax.axis_index("sp"), lax.axis_index("tp")
    c = lax.rem(s, n_c)
    y = lax.rem(s // n_c, n_y)
    z = s // (n_c * n_y)
    far_s = n_sp - 1 - s
    rows = queries_one.shape[0]
    half, block = rows // 2, rows // n_tp
    feats = stream.shape[1]
    turn = n_z // 2
    n_keys = n_y // 2 * n_c * rows
    f32, bf = jnp.float32, jnp.bfloat16

    def sp_of(zz, yy, cc):
        return (zz * n_y + yy) * n_c + cc

    def zn(d):
        return lax.rem(z + d + n_z, n_z)

    def yn(d):
        return lax.rem(y + d + n_y, n_y)

    def tn(d):
        return lax.rem(t + d, n_tp)

    def remote(src, dst, a, b, sp, tp):
        return pltpu.make_async_remote_copy(
            src_ref=src, dst_ref=dst, send_sem=a, recv_sem=b, device_id=(sp, tp), device_id_type=MESH)

    def arrived(ref, sem):
        remote(ref, ref, sent.at[0], sem, far_s, t).wait_recv()

    def left(ref, sem):
        remote(ref, ref, sem, qsem.at[0], far_s, t).wait_send()

    mine = kv.at[z, y, c]
    own = [
        pltpu.make_async_copy(keys_one, mine.at[:, pl.ds(0, HEAD_DIM)], local_sem.at[0]),
        pltpu.make_async_copy(keys_two, mine.at[:, pl.ds(HEAD_DIM, HEAD_DIM)], local_sem.at[1]),
        pltpu.make_async_copy(values, mine.at[:, pl.ds(2 * HEAD_DIM, VAL_DIM)], local_sem.at[2]),
    ]
    for copy in own:
        copy.start()

    barrier = pltpu.get_barrier_semaphore()

    def hello(sp, tp):
        pl.semaphore_signal(barrier, inc=1, device_id=(sp, tp), device_id_type=MESH)

    hello(sp_of(z, y, 1 - c), t)
    for d in (1, -1):
        hello(sp_of(zn(d), y, c), t)
        hello(sp_of(z, yn(d), c), t)
    for d in range(1, n_tp):
        hello(s, tn(d))
    hello(far_s, t)
    for q in range(n_tp // 2, n_tp):
        hello(far_s, q)
    high = t // (n_tp // 2)
    pl.semaphore_wait(barrier, 5 + n_tp + high * n_tp)
    for copy in own:
        copy.wait()

    def lower(zz, yy):
        return kv.at[zz, yy, c, pl.ds(0, split)]

    def upper(zz, yy):
        return kv.at[zz, yy, c, pl.ds(split, rows - split)]

    def to_z(ref, d, a, sem):
        remote(ref, ref, sent.at[a], sem, sp_of(zn(d), y, c), t).start()

    def to_y(ref, d, a, sem):
        remote(ref, ref, sent.at[a], sem, sp_of(z, yn(d), c), t).start()

    for k, d in enumerate((1, -1)):
        to_z(lower(z, y), d, 0, pz.at[k, 1])
        to_y(upper(z, y), d, 1, ry.at[k])
    for i, queries in enumerate((queries_one, queries_two)):
        remote(queries.at[pl.ds(half, half)], q_far.at[i], sent.at[2], qsem.at[i], far_s, t).start()
    for k, d in enumerate((1, -1)):
        to_z(upper(z, y), d, 3, rz.at[0, k, 1])
        to_y(lower(z, y), d, 4, py.at[0, k])

    sp_home = jnp.where(high == 1, far_s, s)
    slab = stream.at[pl.ds(pl.multiple_of(t * block, block), block)]
    for q in range(n_tp):
        piece = stream_in.at[:, pl.ds(q * feats, feats)]
        at_home = (t == q) & (high == 0)

        @pl.when(at_home)
        def _():
            pltpu.make_async_copy(piece, slab, local_sem.at[3]).start()
            pltpu.make_async_copy(meta_in, meta.at[t], local_sem.at[4]).start()

        @pl.when(jnp.logical_not(at_home))
        def _():
            remote(meta_in, meta.at[t], sent.at[5], msem.at[t], sp_home, q).start()
            remote(piece, slab, sent.at[6], ssem.at[t], sp_home, q).start()

    depth, units = out_w.shape[0], down_w.shape[0]
    out_rows = out_cols.at[pl.ds(pl.multiple_of(t * depth, depth), depth)]
    down_rows = down_cols.at[pl.ds(pl.multiple_of(t * units, units), units)]

    def strip(ref, q):
        return ref.at[:, pl.ds(pl.multiple_of(q * feats, feats), feats)]

    for d in range(1, n_tp):
        remote(strip(down_w, tn(d)), down_rows, sent.at[7], wsem.at[d], s, tn(d)).start()
        remote(strip(out_w, tn(d)), out_rows, sent.at[8], osem.at[d], s, tn(d)).start()
    weights = [
        pltpu.make_async_copy(strip(down_w, t), down_rows, local_sem.at[5]),
        pltpu.make_async_copy(strip(out_w, t), out_rows, local_sem.at[6]),
    ]
    for copy in weights:
        copy.start()

    for k, d in enumerate((-1, 1)):
        ref = upper(z, yn(d))
        arrived(ref, ry.at[k])

        @pl.when(c == k)
        def _():
            to_y(ref, -d, 9, ry2.at[0])

        for kk, dd in enumerate((1, -1)):
            to_z(ref, dd, 3, rz.at[1 + k, kk, 1])
    ref = upper(z, yn(2))
    arrived(ref, ry2.at[0])
    for kk, dd in enumerate((1, -1)):
        to_z(ref, dd, 3, rz.at[3, kk, 1])

    m_ref[...] = jnp.full(m_ref.shape, -1e30, f32)
    l_ref[...] = jnp.zeros(l_ref.shape, f32)
    acc_ref[...] = jnp.zeros(acc_ref.shape, f32)

    def plane(j):
        return lax.rem(z + (j + 1) // 2 * (1 - 2 * lax.rem(j, 2)) + n_z, n_z)

    def goes(h, k):
        return (h < turn) | ((h == turn) & (c == k))

    def each_plane(h, f):
        for a in range(2):
            j = jnp.where(h == 0, 0, jnp.minimum(2 * h - 1 + a, n_z - 1))

            @pl.when((a == 0) | ((h >= 1) & (h < turn)))
            def _():
                f(j, plane(j))

    def lower_arrives(h):
        for k, d in enumerate((1, -1)):

            @pl.when(goes(h, k))
            def _():
                zz = zn(-d * h)
                ref = lower(zz, y)
                arrived(ref, pz.at[k, h])

                @pl.when(goes(h + 1, k))
                def _():
                    to_z(ref, d, 0, pz.at[k, h + 1])

                j = jnp.minimum(2 * h - 1 + k, n_z - 1)
                for kk, dd in enumerate((1, -1)):
                    to_y(ref, dd, 4, py.at[j, kk])

    def upper_arrives(h, r):
        yy = lax.rem(y + jnp.where(r == 0, 0, jnp.where(r == 1, n_y - 1, jnp.where(r == 2, 1, 2))), n_y)
        for k, d in enumerate((1, -1)):

            @pl.when(goes(h, k))
            def _():
                ref = upper(zn(-d * h), yy)
                arrived(ref, rz.at[r, k, h])

                @pl.when(goes(h + 1, k))
                def _():
                    to_z(ref, d, 3, rz.at[r, k, h + 1])

    def spread(j, zz):
        arrived(lower(zz, yn(-1)), py.at[j, 0])
        arrived(lower(zz, yn(1)), py.at[j, 1])
        d = 1 - 2 * lax.rem(j, 2)
        to_y(lower(zz, yn(-d)), d, 10, py2.at[j])

    def share(j, zz):
        arrived(lower(zz, yn(2)), py2.at[j])
        ref = kv.at[zz, :, c]
        remote(ref, ref, sent.at[11], sib.at[j], sp_of(z, y, 1 - c), t).start()

    def update(run, zz, part, masked, first_row):
        keys_all = kv[zz, pl.ds(part * (n_y // 2), n_y // 2)].reshape(n_keys, 2 * HEAD_DIM + VAL_DIM)
        v = keys_all[:, 2 * HEAD_DIM :]
        if masked:
            first_key = (zz * 2 + part) * n_keys
            row = first_row + lax.rem(lax.broadcasted_iota(jnp.int32, (rows, n_keys), 0), half)
            keep = first_key + lax.broadcasted_iota(jnp.int32, (rows, n_keys), 1) <= row
        for k in range(2):
            keys = keys_all[:, k * HEAD_DIM : (k + 1) * HEAD_DIM]
            scores = lax.dot_general(q_all[run, k], keys, (((1,), (1,)), ((), ())), preferred_element_type=f32)
            if masked:
                scores = jnp.where(keep, scores, -jnp.inf)
            old = m_ref[run, k]
            new = jnp.maximum(old, jnp.max(scores, axis=1, keepdims=True))
            terms = jnp.exp2((scores - new[:, :1]) * SCALE2)
            fade = jnp.exp2((old - new) * SCALE2)
            lanes = terms[:, :128]
            for i in range(1, n_keys // 128):
                lanes = lanes + terms[:, i * 128 : (i + 1) * 128]
            m_ref[run, k] = new
            l_ref[run, k] = l_ref[run, k] * fade + lanes
            acc_ref[run, k] = acc_ref[run, k] * fade[:, :1] + jnp.dot(terms.astype(bf), v, preferred_element_type=f32)

    def row_of(run):
        return jnp.where(run == 0, s * rows, far_s * rows + half)

    def attend(j, part):
        zz = plane(j)

        @pl.when(part == 0)
        def _():
            arrived(kv.at[zz, :, 1 - c], sib.at[j])

        def one(run, carry):
            here, last = zz * 2 + part, row_of(run) // n_keys

            @pl.when(here < last)
            def _():
                update(run, zz, part, False, row_of(run))

            @pl.when(here == last)
            def _():
                update(run, zz, part, True, row_of(run))

            return carry

        lax.fori_loop(0, 2, one, 0)

    def step(u, carry):
        h, sub = u // 5, lax.rem(u, 5)

        @pl.when((sub == 0) & (h <= turn))
        def _():
            lower_arrives(h)

        @pl.when(sub == 0)
        def _():
            each_plane(h - 1, spread)

        @pl.when((sub > 0) & (h <= turn))
        def _():
            upper_arrives(h, sub - 1)

        @pl.when(sub == 2)
        def _():
            each_plane(h - 1, share)

        @pl.when(u == 8)
        def _():
            for i, queries in enumerate((queries_one, queries_two)):
                arrived(q_far.at[i], qsem.at[i])
                for g in range(2):
                    place = pl.ds(g * half, half)
                    lanes = slice(g * HEAD_DIM, (g + 1) * HEAD_DIM)
                    q_all[0, i, place] = queries[:half, lanes]
                    q_all[1, i, place] = q_far[i, :, lanes]

        v = u - 8
        hc, i = v // 5, lax.rem(v, 5)
        j = jnp.where(hc == 0, 0, jnp.minimum(2 * hc - 1 + i // 2, n_z - 1))

        @pl.when((v >= 0) & ((i < 2) | ((i < 4) & (hc > 0) & (hc < turn))))
        def _():
            attend(j, lax.rem(i, 2))

        return carry

    lax.fori_loop(5, 5 * (turn + 2), step, 0)

    for run in range(2):
        mix = [acc_ref[run, k] / jnp.sum(l_ref[run, k], axis=1, keepdims=True) for k in range(2)]
        for g in range(2):
            piece = slice(g * half, (g + 1) * half)
            diff = mix[0][piece] - lam[g] * mix[1][piece]
            ms = jnp.mean(diff * diff, axis=1, keepdims=True)
            res = diff * lax.rsqrt(ms + EPS) * gain[...] * OUT_SCALE
            heads[run * half : (run + 1) * half, g * VAL_DIM : (g + 1) * VAL_DIM] = res.astype(bf)

    for q in range(n_tp):
        ref = stream.at[pl.ds(q * block, block)]
        at_home = (t == q) & (high == 0)

        @pl.when(at_home)
        def _():
            pltpu.make_async_copy(stream_in.at[:, pl.ds(q * feats, feats)], ref, local_sem.at[3]).wait()
            pltpu.make_async_copy(meta_in, meta.at[q], local_sem.at[4]).wait()

        @pl.when(jnp.logical_not(at_home))
        def _():
            arrived(ref, ssem.at[q])
            arrived(meta.at[q], msem.at[q])

    for copy in weights:
        copy.wait()
    for d in range(1, n_tp):
        arrived(down_rows, wsem.at[d])
        arrived(out_rows, osem.at[d])
    left(kv.at[pl.ds(0, n_z - 1), 0, 0, pl.ds(0, split)], sent.at[0])
    left(kv.at[0, pl.ds(0, 2), 0, pl.ds(split, rows - split)], sent.at[1])
    left(q_far, sent.at[2])
    left(kv.at[pl.ds(0, n_z - 1), :, 0, pl.ds(split, rows - split)], sent.at[3])
    left(kv.at[:, pl.ds(0, 2), 0, pl.ds(0, split)], sent.at[4])
    left(kv.at[0, 0, 0, pl.ds(split, rows - split)], sent.at[9])
    left(kv.at[:, 0, 0, pl.ds(0, split)], sent.at[10])
    left(kv.at[:, :, 0], sent.at[11])
    for d in range(1, n_tp):
        left(down_rows, sent.at[7])
        left(out_rows, sent.at[8])

    @pl.when(high == 0)
    def _():
        left(meta.at[pl.ds(0, n_tp - 1)], sent.at[5])
        left(stream.at[pl.ds(0, (n_tp - 1) * block)], sent.at[6])

    @pl.when(high == 1)
    def _():
        left(meta, sent.at[5])
        left(stream, sent.at[6])


def front(queries_one, queries_two, keys_one, keys_two, values, stream_in, meta, out_w, down_w, lam, gain, dims):
    n_z, n_y, n_c, n_tp, split = dims
    rows = queries_one.shape[0]
    feats = stream_in.shape[1] // n_tp
    turn = n_z // 2
    bf, f32 = jnp.bfloat16, jnp.float32
    dma = pltpu.SemaphoreType.DMA
    vmem, hbm = pl.BlockSpec(memory_space=pltpu.VMEM), pl.BlockSpec(memory_space=pl.ANY)
    smem = pl.BlockSpec(memory_space=pltpu.SMEM)
    return pl.pallas_call(
        functools.partial(front_kernel, dims),
        out_shape=(
            jax.ShapeDtypeStruct((rows, 2 * VAL_DIM), bf),
            jax.ShapeDtypeStruct((rows, feats), bf),
            jax.ShapeDtypeStruct((n_tp,) + meta.shape, f32),
            jax.ShapeDtypeStruct((n_tp * out_w.shape[0], feats), bf),
            jax.ShapeDtypeStruct((n_tp * down_w.shape[0], feats), bf),
        ),
        in_specs=[vmem, vmem, hbm, hbm, hbm, vmem, vmem, hbm, hbm, smem, vmem],
        out_specs=(vmem, vmem, vmem, hbm, hbm),
        scratch_shapes=[
            pltpu.VMEM((n_z, n_y, n_c, rows, 2 * HEAD_DIM + VAL_DIM), bf),
            pltpu.VMEM((2, rows // 2, 2 * HEAD_DIM), bf),
            pltpu.VMEM((2, 2, rows, HEAD_DIM), bf),
            pltpu.VMEM((2, 2, rows, 128), f32),
            pltpu.VMEM((2, 2, rows, 128), f32),
            pltpu.VMEM((2, 2, rows, VAL_DIM), f32),
            dma((12,)), dma((7,)), dma((2,)), dma((n_tp,)), dma((n_tp,)), dma((n_tp,)), dma((n_tp,)),
            dma((2, turn + 1)), dma((n_z, 2)), dma((n_z,)), dma((2,)), dma((1,)), dma((4, 2, turn + 1)), dma((n_z,)),
        ],
        compiler_params=pltpu.CompilerParams(
            collective_id=0, has_side_effects=True, vmem_limit_bytes=48 * 1024 * 1024),
        name="front",
    )(queries_one, queries_two, keys_one, keys_two, values, stream_in, meta, out_w, down_w, lam, gain)


def post_kernel(n_sp, n_tp, group, heads, out_w, stream_in, gain, meta, gate_h, up_h, down_h,
                out, hall, slots_row, slots_col, oc, gate_w, up_w, down_w, stream, ssq, send, xbuf, hbuf, rbuf, back, mix,
                sent, local_sem, wsem, asem, a2sem, qsem, dsem, xsem, x2sem, hsem, h2sem, bsem, fsem):
    s, t = lax.axis_index("sp"), lax.axis_index("tp")
    n_z = n_sp // group
    z, w = s // group, lax.rem(s, group)
    far_s = n_sp - 1 - s
    cap, feats = send.shape[1], send.shape[2]
    units = gate_w.shape[1]
    rows = heads.shape[0]
    half, block = rows // 2, rows // n_tp
    f32, bf = jnp.float32, jnp.bfloat16

    loads = [
        pltpu.make_async_copy(a, b, wsem.at[i])
        for i, (a, b) in enumerate(((out_w, oc), (gate_h, gate_w), (up_h, up_w), (down_h, down_w)))
    ]
    for load in loads:
        load.start()

    def side(d):
        return lax.rem(t + d + n_tp, n_tp)

    def offset(j):
        away = (n_z // 2 - j // 2) * jnp.minimum(j, 1)
        return away * (1 - 2 * lax.rem(j, 2))

    def to_plane(j):
        return lax.rem(z + offset(j) + n_z, n_z)

    def from_plane(j):
        return lax.rem(z - offset(j) + n_z, n_z)

    def remote(src, dst, a, b, sp, tp):
        return pltpu.make_async_remote_copy(
            src_ref=src, dst_ref=dst, send_sem=a, recv_sem=b, device_id=(sp, tp), device_id_type=MESH)

    def arrived(ref, sem):
        remote(ref, ref, sent.at[0], sem, s, side(1)).wait_recv()

    def left(ref, sem):
        remote(ref, ref, sem, dsem.at[0], s, side(1)).wait_send()

    barrier = pltpu.get_barrier_semaphore()

    def hello(sp, tp):
        pl.semaphore_signal(barrier, inc=1, device_id=(sp, tp), device_id_type=MESH)

    def greet(o, c):
        hello(lax.rem(s + o, n_sp), t)
        return c

    lax.fori_loop(1, n_sp, greet, 0)
    for d in range(1, n_tp):
        hello(s, side(d))
    low = t < n_tp // 2

    @pl.when(jnp.logical_not(low))
    def _():
        for d in range(n_tp):
            hello(far_s, d)

    pl.semaphore_wait(barrier, n_sp - 1 + n_tp - 1 + n_tp // 2)

    for k, d in enumerate((1, -1)):
        remote(heads, hall.at[t], sent.at[6], asem.at[k], s, side(d)).start()

    base = jnp.concatenate([jnp.concatenate([meta[q]] * 16, axis=0).T[:block] for q in range(n_tp)], axis=0)
    lane = lax.broadcasted_iota(jnp.int32, (rows, 128), 1)
    earlier = lax.broadcasted_iota(jnp.int32, (rows, rows), 1) < lax.broadcasted_iota(jnp.int32, (rows, rows), 0)
    earlier = jnp.where(earlier, 1.0, 0.0).astype(bf)
    taken = jnp.zeros((1, 128), f32)
    places = base
    for k in range(2):
        named = jnp.where(lane.astype(f32) == base[:, k : k + 1], 1.0, 0.0)
        before = jnp.dot(earlier, named.astype(bf), preferred_element_type=f32) + taken
        rank = jnp.sum(before * named, axis=1, keepdims=True)
        taken = taken + jnp.sum(named, axis=0, keepdims=True)
        places = jnp.where(lane == k, base[:, k : k + 1] * cap + rank, places)
    slots_col[...] = places
    slots_row[...] = places.T[:8]
    loads[0].wait()

    width = heads.shape[1]

    def project(x, q):
        return jnp.dot(x, oc[pl.ds(pl.multiple_of(q * width, width), width)], preferred_element_type=f32)

    stream[...] = stream_in[...].astype(f32) + project(heads[...], t)
    for k, d in enumerate((-1, 1)):
        arrived(hall.at[side(d)], asem.at[k])
        ref = hall.at[side(d), pl.ds(k * half, half)]
        remote(ref, ref, sent.at[7], a2sem.at[k], s, side(-d)).start()
    stream[...] += project(hall[side(-1)], side(-1)) + project(hall[side(1)], side(1))
    for k in range(2):
        arrived(hall.at[side(2), pl.ds(k * half, half)], a2sem.at[k])
    total = stream[...] + project(hall[side(2)], side(2))
    stream[...] = total

    part = jnp.sum(total * total, axis=1, keepdims=True)
    ssq[t] = jnp.broadcast_to(part, (rows, 128)).T[:8]
    for d in range(1, n_tp):
        remote(ssq.at[t], ssq.at[t], sent.at[8], qsem.at[d], s, side(d)).start()
    for d in range(1, n_tp):
        arrived(ssq.at[side(-d)], qsem.at[d])
    sums = ssq[0]
    for q in range(1, n_tp):
        sums = sums + ssq[q]
    inv = lax.rsqrt(sums / (feats * n_tp) + EPS)
    inv = jnp.concatenate([inv] * 16, axis=0).T[:, :1]
    normed = (stream[...] * inv * gain[:, pl.ds(pl.multiple_of(t * feats, feats), feats)]).astype(bf)

    own = pltpu.make_async_copy(send.at[s], xbuf.at[t, s], local_sem.at[0])

    def pack(j):
        plane = to_plane(j)
        place = plane * (group * cap) + lax.broadcasted_iota(jnp.int32, (group * cap, rows), 0)
        place = place.astype(f32)
        chosen = (place == slots_row[0:1, :]) | (place == slots_row[1:2, :])
        picked = jnp.dot(jnp.where(chosen, 1.0, 0.0).astype(bf), normed, preferred_element_type=f32)
        send[pl.ds(pl.multiple_of(plane * group, group), group)] = picked.astype(bf).reshape(group, cap, feats)
        return plane

    pack(0)
    own.start()

    def near(i, c):
        dest = z * group + lax.rem(w + i, group)
        remote(send.at[dest], xbuf.at[t, s], sent.at[0], dsem.at[0], dest, t).start()
        return c

    lax.fori_loop(1, group, near, 0)

    def far(j, c):
        plane = pack(j)

        def one(i, c):
            dest = plane * group + lax.rem(w + i, group)
            remote(send.at[dest], xbuf.at[t, s], sent.at[0], dsem.at[j], dest, t).start()
            return c

        return lax.fori_loop(0, group, one, c)

    lax.fori_loop(1, n_z, far, 0)
    for load in loads[1:]:
        load.wait()

    def chunk(q, j):
        return xbuf.at[q, pl.ds(from_plane(j) * group, group)]

    def stage_x(j):
        @pl.when(j == 0)
        def _():
            own.wait()
            arrived(xbuf.at[t, pl.ds(0, group - 1)], dsem.at[0])

        @pl.when(j > 0)
        def _():
            arrived(chunk(t, j), dsem.at[j])

        for k, d in enumerate((1, -1)):
            remote(chunk(t, j), chunk(t, j), sent.at[1], xsem.at[k, j], s, side(d)).start()

    def stage_x2(j):
        arrived(chunk(side(-1), j), xsem.at[0, j])
        arrived(chunk(side(1), j), xsem.at[1, j])
        d = 1 - 2 * lax.rem(j, 2)
        ref = chunk(side(-d), j)
        remote(ref, ref, sent.at[2], x2sem.at[j], s, side(d)).start()

    def stage_up(j):
        arrived(chunk(side(2), j), x2sem.at[j])
        first = pl.multiple_of(from_plane(j) * group, group)
        gate = jnp.zeros((group * cap, units), f32)
        upper = jnp.zeros((group * cap, units), f32)
        for q in range(n_tp):
            x = xbuf[q, pl.ds(first, group)].reshape(group * cap, feats)
            gate = gate + jnp.dot(x, gate_w[q * feats : (q + 1) * feats], preferred_element_type=f32)
            upper = upper + jnp.dot(x, up_w[q * feats : (q + 1) * feats], preferred_element_type=f32)
        act = gate / (1.0 + jnp.exp(-gate)) * upper
        plane = from_plane(j)
        hbuf[t, plane] = act.astype(bf)
        for k, d in enumerate((1, -1)):
            ref = hbuf.at[t, plane]
            remote(ref, ref, sent.at[3], hsem.at[k, j], s, side(d)).start()

    def stage_h2(j):
        plane = from_plane(j)
        arrived(hbuf.at[side(-1), plane], hsem.at[0, j])
        arrived(hbuf.at[side(1), plane], hsem.at[1, j])
        d = 1 - 2 * lax.rem(j, 2)
        ref = hbuf.at[side(-d), plane]
        remote(ref, ref, sent.at[4], h2sem.at[j], s, side(d)).start()

    def stage_down(j):
        plane = from_plane(j)
        arrived(hbuf.at[side(2), plane], h2sem.at[j])
        res = jnp.zeros((group * cap, feats), f32)
        for q in range(n_tp):
            res = res + jnp.dot(hbuf[q, plane], down_w[q * units : (q + 1) * units], preferred_element_type=f32)
        first = pl.multiple_of(plane * group, group)
        rbuf[pl.ds(first, group)] = res.astype(bf).reshape(group, cap, feats)

        @pl.when(j == 0)
        def _():
            pltpu.make_async_copy(rbuf.at[s], back.at[s], local_sem.at[1]).start()

            def one(i, c):
                dest = z * group + lax.rem(w + i, group)
                remote(rbuf.at[dest], back.at[s], sent.at[5], bsem.at[0], dest, t).start()
                return c

            lax.fori_loop(1, group, one, 0)

        @pl.when(j > 0)
        def _():
            def one(i, c):
                dest = plane * group + lax.rem(w + i, group)
                remote(rbuf.at[dest], back.at[s], sent.at[5], bsem.at[j], dest, t).start()
                return c

            lax.fori_loop(0, group, one, 0)

    stages = (stage_x, stage_x2, stage_up, stage_h2, stage_down)

    def step(i, c):
        for lag, stage in enumerate(stages):
            j = i - lag

            @pl.when((j >= 0) & (j < n_z))
            def _():
                stage(j)

        return c

    lax.fori_loop(0, n_z + len(stages) - 1, step, 0)

    pltpu.make_async_copy(rbuf.at[s], back.at[s], local_sem.at[1]).wait()
    arrived(back.at[pl.ds(0, group - 1)], bsem.at[0])

    def home(j, c):
        arrived(back.at[pl.ds(to_plane(j) * group, group)], bsem.at[j])
        return c

    lax.fori_loop(1, n_z, home, 0)

    table = back[...].reshape(n_sp * cap, feats)
    total = stream[...]
    place = lax.broadcasted_iota(jnp.int32, (rows, n_sp * cap), 1).astype(f32)
    for k in range(2):
        chosen = jnp.where(place == slots_col[:, k : k + 1], 1.0, 0.0).astype(bf)
        total = total + slots_col[:, 2 + k : 3 + k] * jnp.dot(chosen, table, preferred_element_type=f32)
    mix[...] = total.astype(bf)
    columns = out.at[:, pl.ds(pl.multiple_of(t * feats, feats), feats)]
    for b in range(n_tp):
        piece = mix.at[pl.ds(b * block, block)]
        if b < n_tp // 2:

            @pl.when(t == b)
            def _():
                pltpu.make_async_copy(piece, columns, local_sem.at[2]).start()

            @pl.when(t != b)
            def _():
                remote(piece, columns, sent.at[9], fsem.at[t], s, b).start()
        else:
            remote(piece, columns, sent.at[9], fsem.at[t], far_s, b).start()
    for q in range(n_tp):
        ref = out.at[:, pl.ds(q * feats, feats)]
        mine = (t == q) & low

        @pl.when(mine)
        def _():
            pltpu.make_async_copy(mix.at[pl.ds(0, block)], ref, local_sem.at[2]).wait()

        @pl.when(jnp.logical_not(mine))
        def _():
            arrived(ref, fsem.at[q])

    left(send.at[pl.ds(0, n_sp - 1)], sent.at[0])
    left(xbuf.at[pl.ds(0, 2)], sent.at[1])
    left(xbuf.at[0], sent.at[2])
    left(hbuf.at[pl.ds(0, 2)], sent.at[3])
    left(hbuf.at[0], sent.at[4])
    left(rbuf.at[pl.ds(0, n_sp - 1)], sent.at[5])
    left(hall.at[pl.ds(0, 2)], sent.at[6])
    left(hall.at[0], sent.at[7])
    left(ssq.at[pl.ds(0, n_tp - 1)], sent.at[8])

    @pl.when(low)
    def _():
        left(mix.at[pl.ds(0, (n_tp - 1) * block)], sent.at[9])

    @pl.when(jnp.logical_not(low))
    def _():
        left(mix, sent.at[9])


def post(heads, out_w, stream_in, gain, meta, gate_w, up_w, down_w, n_sp, n_tp, group, cap):
    rows, feats = stream_in.shape
    units = gate_w.shape[1]
    n_z = n_sp // group
    bf, f32 = jnp.bfloat16, jnp.float32
    dma = pltpu.SemaphoreType.DMA
    vmem, hbm = pl.BlockSpec(memory_space=pltpu.VMEM), pl.BlockSpec(memory_space=pl.ANY)
    return pl.pallas_call(
        functools.partial(post_kernel, n_sp, n_tp, group),
        out_shape=jax.ShapeDtypeStruct((rows // n_tp, feats * n_tp), bf),
        in_specs=[vmem, hbm, vmem, vmem, vmem, hbm, hbm, hbm],
        out_specs=vmem,
        scratch_shapes=[
            pltpu.VMEM((n_tp,) + heads.shape, bf),
            pltpu.VMEM((8, rows), f32),
            pltpu.VMEM((rows, 128), f32),
            pltpu.VMEM(out_w.shape, bf),
            pltpu.VMEM(gate_w.shape, bf),
            pltpu.VMEM(up_w.shape, bf),
            pltpu.VMEM(down_w.shape, bf),
            pltpu.VMEM((rows, feats), f32),
            pltpu.VMEM((n_tp, 8, rows), f32),
            pltpu.VMEM((n_sp, cap, feats), bf),
            pltpu.VMEM((n_tp, n_sp, cap, feats), bf),
            pltpu.VMEM((n_tp, n_z, group * cap, units), bf),
            pltpu.VMEM((n_sp, cap, feats), bf),
            pltpu.VMEM((n_sp, cap, feats), bf),
            pltpu.VMEM((rows, feats), bf),
            dma((10,)), dma((3,)), dma((4,)), dma((2,)), dma((2,)), dma((n_tp,)), dma((n_z,)), dma((2, n_z)),
            dma((n_z,)), dma((2, n_z)), dma((n_z,)), dma((n_z,)), dma((n_tp,)),
        ],
        compiler_params=pltpu.CompilerParams(
            collective_id=1, has_side_effects=True, vmem_limit_bytes=40 * 1024 * 1024),
        name="post",
    )(heads, out_w, stream_in, gain, meta, gate_w, up_w, down_w)


def shards(
    stream_in, queries_one, queries_two, keys_one, keys_two, values, lambdas, head_gain, out_weight,
    norm_gain, expert_ids, route_weight, gate_weight, up_weight, down_weight,
):
    n_sp, n_tp = lax.axis_size("sp"), lax.axis_size("tp")
    meta = jnp.concatenate([expert_ids.astype(jnp.float32), route_weight], 1).T
    meta = jnp.pad(meta, ((0, 8 - meta.shape[0]), (0, 128 - meta.shape[1])))
    heads, stream, meta, out_cols, down_cols = front(
        queries_one, queries_two, keys_one, keys_two, values, stream_in, meta, out_weight, down_weight[0],
        lambdas, head_gain[None], CHIPS + (n_tp, SPLIT),
    )
    return post(
        heads, out_cols, stream, norm_gain[None], meta, gate_weight[0], up_weight[0], down_cols,
        n_sp, n_tp, n_sp // CHIPS[0], CAP,
    )


def solution(mesh):
    return jax.shard_map(
        shards,
        mesh=mesh,
        in_specs=(
            P(("sp", "tp"), None),
            P("sp", "tp"),
            P("sp", "tp"),
            P("sp", "tp"),
            P("sp", "tp"),
            P("sp", "tp"),
            P("tp"),
            P(),
            P("tp", None),
            P(),
            P(("sp", "tp"), None),
            P(("sp", "tp"), None),
            P("sp", None, "tp"),
            P("sp", None, "tp"),
            P("sp", "tp", None),
        ),
        out_specs=P(("sp", "tp"), None),
        check_vma=False,
    )
```

```python
import functools
import math

import jax
import jax.numpy as jnp
from jax import lax
from jax.experimental import pallas as pl
from jax.experimental.pallas import tpu as pltpu
from jax.sharding import PartitionSpec as P

HEAD_DIM = 128
VAL_DIM = 256
EPS = 1e-06
OUT_SCALE = 0.8
SCALE2 = HEAD_DIM ** (-0.5) * math.log2(math.e)
MESH = pl.DeviceIdType.MESH
CHIPS = (8, 4, 2)
SPLIT = 144
CAP = 16
LAST = 14


def front_kernel(dims, queries_one, queries_two, keys_one, keys_two, values, stream_in, meta_in, out_w, down_w, lam, gain,
                 heads, stream, meta, out_cols, down_cols, kv, q_far, q_all, m_ref, l_ref, acc_ref,
                 sent, local_sem, qsem, ssem, msem, osem, wsem, pz, py, py2, ry, ry2, rz, sib):
    n_z, n_y, n_c, n_tp, split = dims
    n_sp = n_z * n_y * n_c
    s, t = lax.axis_index("sp"), lax.axis_index("tp")
    c = lax.rem(s, n_c)
    y = lax.rem(s // n_c, n_y)
    z = s // (n_c * n_y)
    far_s = n_sp - 1 - s
    rows = queries_one.shape[0]
    half, block = rows // 2, rows // n_tp
    feats = stream.shape[1]
    turn = n_z // 2
    n_keys = n_y // 2 * n_c * rows
    f32, bf = jnp.float32, jnp.bfloat16

    def sp_of(zz, yy, cc):
        return (zz * n_y + yy) * n_c + cc

    def zn(d):
        return lax.rem(z + d + n_z, n_z)

    def yn(d):
        return lax.rem(y + d + n_y, n_y)

    def tn(d):
        return lax.rem(t + d, n_tp)

    def remote(src, dst, a, b, sp, tp):
        return pltpu.make_async_remote_copy(
            src_ref=src, dst_ref=dst, send_sem=a, recv_sem=b, device_id=(sp, tp), device_id_type=MESH)

    def arrived(ref, sem):
        remote(ref, ref, sent.at[0], sem, far_s, t).wait_recv()

    def left(ref, sem):
        remote(ref, ref, sem, qsem.at[0], far_s, t).wait_send()

    mine = kv.at[z, y, c]
    own = [
        pltpu.make_async_copy(keys_one, mine.at[:, pl.ds(0, HEAD_DIM)], local_sem.at[0]),
        pltpu.make_async_copy(keys_two, mine.at[:, pl.ds(HEAD_DIM, HEAD_DIM)], local_sem.at[1]),
        pltpu.make_async_copy(values, mine.at[:, pl.ds(2 * HEAD_DIM, VAL_DIM)], local_sem.at[2]),
    ]
    for copy in own:
        copy.start()

    barrier = pltpu.get_barrier_semaphore()

    def hello(sp, tp):
        pl.semaphore_signal(barrier, inc=1, device_id=(sp, tp), device_id_type=MESH)

    hello(sp_of(z, y, 1 - c), t)
    for d in (1, -1):
        hello(sp_of(zn(d), y, c), t)
        hello(sp_of(z, yn(d), c), t)
    for d in range(1, n_tp):
        hello(s, tn(d))
    hello(far_s, t)
    for q in range(n_tp // 2, n_tp):
        hello(far_s, q)
    high = t // (n_tp // 2)
    pl.semaphore_wait(barrier, 5 + n_tp + high * n_tp)
    for copy in own:
        copy.wait()

    def lower(zz, yy):
        return kv.at[zz, yy, c, pl.ds(0, split)]

    def upper(zz, yy):
        return kv.at[zz, yy, c, pl.ds(split, rows - split)]

    def to_z(ref, d, a, sem):
        remote(ref, ref, sent.at[a], sem, sp_of(zn(d), y, c), t).start()

    def to_y(ref, d, a, sem):
        remote(ref, ref, sent.at[a], sem, sp_of(z, yn(d), c), t).start()

    for k, d in enumerate((1, -1)):
        to_z(lower(z, y), d, 0, pz.at[k, 1])
        to_y(upper(z, y), d, 1, ry.at[k])
    for i, queries in enumerate((queries_one, queries_two)):
        remote(queries.at[pl.ds(half, half)], q_far.at[i], sent.at[2], qsem.at[i], far_s, t).start()
    for k, d in enumerate((1, -1)):
        to_z(upper(z, y), d, 3, rz.at[0, k, 1])
        to_y(lower(z, y), d, 4, py.at[0, k])

    sp_home = jnp.where(high == 1, far_s, s)
    slab = stream.at[pl.ds(pl.multiple_of(t * block, block), block)]

    def send_rows():
        for q in range(n_tp):
            piece = stream_in.at[:, pl.ds(q * feats, feats)]
            at_home = (t == q) & (high == 0)

            @pl.when(at_home)
            def _():
                pltpu.make_async_copy(piece, slab, local_sem.at[3]).start()
                pltpu.make_async_copy(meta_in, meta.at[t], local_sem.at[4]).start()

            @pl.when(jnp.logical_not(at_home))
            def _():
                remote(meta_in, meta.at[t], sent.at[5], msem.at[t], sp_home, q).start()
                remote(piece, slab, sent.at[6], ssem.at[t], sp_home, q).start()

    depth, units = out_w.shape[0], down_w.shape[0]
    out_rows = out_cols.at[pl.ds(pl.multiple_of(t * depth, depth), depth)]
    down_rows = down_cols.at[pl.ds(pl.multiple_of(t * units, units), units)]

    def strip(ref, q):
        return ref.at[:, pl.ds(pl.multiple_of(q * feats, feats), feats)]

    for d in range(1, n_tp):
        remote(strip(down_w, tn(d)), down_rows, sent.at[7], wsem.at[d], s, tn(d)).start()
        remote(strip(out_w, tn(d)), out_rows, sent.at[8], osem.at[d], s, tn(d)).start()
    weights = [
        pltpu.make_async_copy(strip(down_w, t), down_rows, local_sem.at[5]),
        pltpu.make_async_copy(strip(out_w, t), out_rows, local_sem.at[6]),
    ]
    for copy in weights:
        copy.start()

    for k, d in enumerate((-1, 1)):
        ref = upper(z, yn(d))
        arrived(ref, ry.at[k])

        @pl.when(c == k)
        def _():
            to_y(ref, -d, 9, ry2.at[0])

        for kk, dd in enumerate((1, -1)):
            to_z(ref, dd, 3, rz.at[1 + k, kk, 1])
    ref = upper(z, yn(2))
    arrived(ref, ry2.at[0])
    for kk, dd in enumerate((1, -1)):
        to_z(ref, dd, 3, rz.at[3, kk, 1])

    m_ref[...] = jnp.full(m_ref.shape, -1e30, f32)
    l_ref[...] = jnp.zeros(l_ref.shape, f32)
    acc_ref[...] = jnp.zeros(acc_ref.shape, f32)

    def plane(j):
        return lax.rem(z + (j + 1) // 2 * (1 - 2 * lax.rem(j, 2)) + n_z, n_z)

    def goes(h, k):
        return (h < turn) | ((h == turn) & (c == k))

    def each_plane(h, f):
        for a in range(2):
            j = jnp.where(h == 0, 0, jnp.minimum(2 * h - 1 + a, n_z - 1))

            @pl.when((a == 0) | ((h >= 1) & (h < turn)))
            def _():
                f(j, plane(j))

    def lower_arrives(h):
        for k, d in enumerate((1, -1)):

            @pl.when(goes(h, k))
            def _():
                zz = zn(-d * h)
                ref = lower(zz, y)
                arrived(ref, pz.at[k, h])

                @pl.when(goes(h + 1, k))
                def _():
                    to_z(ref, d, 0, pz.at[k, h + 1])

                j = jnp.minimum(2 * h - 1 + k, n_z - 1)
                for kk, dd in enumerate((1, -1)):
                    to_y(ref, dd, 4, py.at[j, kk])

    def upper_arrives(h, r):
        yy = lax.rem(y + jnp.where(r == 0, 0, jnp.where(r == 1, n_y - 1, jnp.where(r == 2, 1, 2))), n_y)
        for k, d in enumerate((1, -1)):

            @pl.when(goes(h, k))
            def _():
                ref = upper(zn(-d * h), yy)
                arrived(ref, rz.at[r, k, h])

                @pl.when(goes(h + 1, k))
                def _():
                    to_z(ref, d, 3, rz.at[r, k, h + 1])

    def spread(j, zz):
        arrived(lower(zz, yn(-1)), py.at[j, 0])
        arrived(lower(zz, yn(1)), py.at[j, 1])
        d = 1 - 2 * lax.rem(j, 2)
        to_y(lower(zz, yn(-d)), d, 10, py2.at[j])

    def share(j, zz):
        arrived(lower(zz, yn(2)), py2.at[j])
        ref = kv.at[zz, :, c]
        remote(ref, ref, sent.at[11], sib.at[j], sp_of(z, y, 1 - c), t).start()

    def update(run, zz, part, masked, first_row):
        keys_all = kv[zz, pl.ds(part * (n_y // 2), n_y // 2)].reshape(n_keys, 2 * HEAD_DIM + VAL_DIM)
        v = keys_all[:, 2 * HEAD_DIM :]
        if masked:
            first_key = (zz * 2 + part) * n_keys
            row = first_row + lax.rem(lax.broadcasted_iota(jnp.int32, (rows, n_keys), 0), half)
            keep = first_key + lax.broadcasted_iota(jnp.int32, (rows, n_keys), 1) <= row
        for k in range(2):
            keys = keys_all[:, k * HEAD_DIM : (k + 1) * HEAD_DIM]
            scores = lax.dot_general(q_all[run, k], keys, (((1,), (1,)), ((), ())), preferred_element_type=f32)
            if masked:
                scores = jnp.where(keep, scores, -jnp.inf)
            old = m_ref[run, k]
            new = jnp.maximum(old, jnp.max(scores, axis=1, keepdims=True))
            terms = jnp.exp2((scores - new[:, :1]) * SCALE2)
            fade = jnp.exp2((old - new) * SCALE2)
            lanes = terms[:, :128]
            for i in range(1, n_keys // 128):
                lanes = lanes + terms[:, i * 128 : (i + 1) * 128]
            m_ref[run, k] = new
            l_ref[run, k] = l_ref[run, k] * fade + lanes
            acc_ref[run, k] = acc_ref[run, k] * fade[:, :1] + jnp.dot(terms.astype(bf), v, preferred_element_type=f32)

    def row_of(run):
        return jnp.where(run == 0, s * rows, far_s * rows + half)

    def blocks(run, j):
        return jnp.clip(row_of(run) // n_keys - 2 * plane(j) + 1, 0, 2)

    def attend(n, u):
        at, base = jnp.int32(0), jnp.int32(0)
        count = jnp.int32(0)
        for j in range(n_z):
            count = count + blocks(0, j) + blocks(1, j)
            passed = count <= n
            at = at + jnp.where(passed, 1, 0)
            base = jnp.where(passed, count, base)
        at = jnp.minimum(at, n_z - 1)
        i = n - base
        short = blocks(0, at)
        run = jnp.where(i < short, 0, 1)
        part = i - jnp.where(i < short, 0, short)
        zz = plane(at)

        ready = (n < 2 * n_z + 1) & (u >= 5 * ((at + 1) // 2) + 7)

        @pl.when(ready & (i == 0))
        def _():
            arrived(kv.at[zz, :, 1 - c], sib.at[at])

        here, last = zz * 2 + part, row_of(run) // n_keys

        @pl.when(ready & (here < last))
        def _():
            update(run, zz, part, False, row_of(run))

        @pl.when(ready & (here == last))
        def _():
            update(run, zz, part, True, row_of(run))

        return n + jnp.where(ready, 1, 0)

    spread(jnp.int32(0), z)

    def step(u, done):
        h, sub = u // 5, lax.rem(u, 5)

        @pl.when((sub == 0) & (h <= turn))
        def _():
            lower_arrives(h)

        @pl.when((sub > 0) & (h <= turn))
        def _():
            upper_arrives(h, sub - 1)

        @pl.when((sub == 3) & (h <= turn))
        def _():
            each_plane(h, spread)

        @pl.when((sub == 1) & (h <= turn + 1))
        def _():
            each_plane(h - 1, share)

        @pl.when(u == 5 * turn)
        def _():
            send_rows()

        @pl.when(u == 6)
        def _():
            for i, queries in enumerate((queries_one, queries_two)):
                arrived(q_far.at[i], qsem.at[i])
                for g in range(2):
                    place = pl.ds(g * half, half)
                    lanes = slice(g * HEAD_DIM, (g + 1) * HEAD_DIM)
                    q_all[0, i, place] = queries[:half, lanes]
                    q_all[1, i, place] = q_far[i, :, lanes]

        return attend(done, u)

    lax.fori_loop(5, 5 * turn + LAST, step, jnp.int32(0))
    for j in range(1, n_z):

        @pl.when(blocks(0, j) + blocks(1, j) == 0)
        def _():
            arrived(kv.at[plane(j), :, 1 - c], sib.at[j])

    for run in range(2):
        mix = [acc_ref[run, k] / jnp.sum(l_ref[run, k], axis=1, keepdims=True) for k in range(2)]
        for g in range(2):
            piece = slice(g * half, (g + 1) * half)
            diff = mix[0][piece] - lam[g] * mix[1][piece]
            ms = jnp.mean(diff * diff, axis=1, keepdims=True)
            res = diff * lax.rsqrt(ms + EPS) * gain[...] * OUT_SCALE
            heads[run * half : (run + 1) * half, g * VAL_DIM : (g + 1) * VAL_DIM] = res.astype(bf)

    for q in range(n_tp):
        ref = stream.at[pl.ds(q * block, block)]
        at_home = (t == q) & (high == 0)

        @pl.when(at_home)
        def _():
            pltpu.make_async_copy(stream_in.at[:, pl.ds(q * feats, feats)], ref, local_sem.at[3]).wait()
            pltpu.make_async_copy(meta_in, meta.at[q], local_sem.at[4]).wait()

        @pl.when(jnp.logical_not(at_home))
        def _():
            arrived(ref, ssem.at[q])
            arrived(meta.at[q], msem.at[q])

    for copy in weights:
        copy.wait()
    for d in range(1, n_tp):
        arrived(down_rows, wsem.at[d])
        arrived(out_rows, osem.at[d])
    left(kv.at[pl.ds(0, n_z - 1), 0, 0, pl.ds(0, split)], sent.at[0])
    left(kv.at[0, pl.ds(0, 2), 0, pl.ds(split, rows - split)], sent.at[1])
    left(q_far, sent.at[2])
    left(kv.at[pl.ds(0, n_z - 1), :, 0, pl.ds(split, rows - split)], sent.at[3])
    left(kv.at[:, pl.ds(0, 2), 0, pl.ds(0, split)], sent.at[4])
    left(kv.at[0, 0, 0, pl.ds(split, rows - split)], sent.at[9])
    left(kv.at[:, 0, 0, pl.ds(0, split)], sent.at[10])
    left(kv.at[:, :, 0], sent.at[11])
    for d in range(1, n_tp):
        left(down_rows, sent.at[7])
        left(out_rows, sent.at[8])

    @pl.when(high == 0)
    def _():
        left(meta.at[pl.ds(0, n_tp - 1)], sent.at[5])
        left(stream.at[pl.ds(0, (n_tp - 1) * block)], sent.at[6])

    @pl.when(high == 1)
    def _():
        left(meta, sent.at[5])
        left(stream, sent.at[6])


def front(queries_one, queries_two, keys_one, keys_two, values, stream_in, meta, out_w, down_w, lam, gain, dims):
    n_z, n_y, n_c, n_tp, split = dims
    rows = queries_one.shape[0]
    feats = stream_in.shape[1] // n_tp
    turn = n_z // 2
    bf, f32 = jnp.bfloat16, jnp.float32
    dma = pltpu.SemaphoreType.DMA
    vmem, hbm = pl.BlockSpec(memory_space=pltpu.VMEM), pl.BlockSpec(memory_space=pl.ANY)
    smem = pl.BlockSpec(memory_space=pltpu.SMEM)
    return pl.pallas_call(
        functools.partial(front_kernel, dims),
        out_shape=(
            jax.ShapeDtypeStruct((rows, 2 * VAL_DIM), bf),
            jax.ShapeDtypeStruct((rows, feats), bf),
            jax.ShapeDtypeStruct((n_tp,) + meta.shape, f32),
            jax.ShapeDtypeStruct((n_tp * out_w.shape[0], feats), bf),
            jax.ShapeDtypeStruct((n_tp * down_w.shape[0], feats), bf),
        ),
        in_specs=[vmem, vmem, hbm, hbm, hbm, vmem, vmem, hbm, hbm, smem, vmem],
        out_specs=(vmem, vmem, vmem, hbm, hbm),
        scratch_shapes=[
            pltpu.VMEM((n_z, n_y, n_c, rows, 2 * HEAD_DIM + VAL_DIM), bf),
            pltpu.VMEM((2, rows // 2, 2 * HEAD_DIM), bf),
            pltpu.VMEM((2, 2, rows, HEAD_DIM), bf),
            pltpu.VMEM((2, 2, rows, 128), f32),
            pltpu.VMEM((2, 2, rows, 128), f32),
            pltpu.VMEM((2, 2, rows, VAL_DIM), f32),
            dma((12,)), dma((7,)), dma((2,)), dma((n_tp,)), dma((n_tp,)), dma((n_tp,)), dma((n_tp,)),
            dma((2, turn + 1)), dma((n_z, 2)), dma((n_z,)), dma((2,)), dma((1,)), dma((4, 2, turn + 1)), dma((n_z,)),
        ],
        compiler_params=pltpu.CompilerParams(
            collective_id=0, has_side_effects=True, vmem_limit_bytes=60 * 1024 * 1024),
        name="front",
    )(queries_one, queries_two, keys_one, keys_two, values, stream_in, meta, out_w, down_w, lam, gain)


def post_kernel(n_sp, n_tp, group, heads, out_w, stream_in, gain, meta, gate_h, up_h, down_h,
                out, hall, slots_row, slots_col, oc, gate_w, up_w, down_w, stream, ssq, send, xbuf, hbuf, rbuf, back, mix,
                sent, local_sem, wsem, asem, a2sem, qsem, dsem, xsem, x2sem, hsem, h2sem, bsem, fsem):
    s, t = lax.axis_index("sp"), lax.axis_index("tp")
    n_z = n_sp // group
    z, w = s // group, lax.rem(s, group)
    far_s = n_sp - 1 - s
    cap, feats = send.shape[1], send.shape[2]
    units = gate_w.shape[1]
    rows = heads.shape[0]
    half, block = rows // 2, rows // n_tp
    f32, bf = jnp.float32, jnp.bfloat16

    loads = [
        pltpu.make_async_copy(a, b, wsem.at[i])
        for i, (a, b) in enumerate(((out_w, oc), (gate_h, gate_w), (up_h, up_w), (down_h, down_w)))
    ]
    for load in loads:
        load.start()

    def side(d):
        return lax.rem(t + d + n_tp, n_tp)

    def offset(j):
        away = (n_z // 2 - j // 2) * jnp.minimum(j, 1)
        return away * (1 - 2 * lax.rem(j, 2))

    def to_plane(j):
        return lax.rem(z + offset(j) + n_z, n_z)

    def from_plane(j):
        return lax.rem(z - offset(j) + n_z, n_z)

    def remote(src, dst, a, b, sp, tp):
        return pltpu.make_async_remote_copy(
            src_ref=src, dst_ref=dst, send_sem=a, recv_sem=b, device_id=(sp, tp), device_id_type=MESH)

    def arrived(ref, sem):
        remote(ref, ref, sent.at[0], sem, s, side(1)).wait_recv()

    def left(ref, sem):
        remote(ref, ref, sem, dsem.at[0], s, side(1)).wait_send()

    barrier = pltpu.get_barrier_semaphore()

    def hello(sp, tp):
        pl.semaphore_signal(barrier, inc=1, device_id=(sp, tp), device_id_type=MESH)

    def greet(o, c):
        hello(lax.rem(s + o, n_sp), t)
        return c

    lax.fori_loop(1, n_sp, greet, 0)
    for d in range(1, n_tp):
        hello(s, side(d))
    low = t < n_tp // 2

    @pl.when(jnp.logical_not(low))
    def _():
        for d in range(n_tp):
            hello(far_s, d)

    pl.semaphore_wait(barrier, n_sp - 1 + n_tp - 1 + n_tp // 2)

    for k, d in enumerate((1, -1)):
        remote(heads, hall.at[t], sent.at[6], asem.at[k], s, side(d)).start()

    base = jnp.concatenate([jnp.concatenate([meta[q]] * 16, axis=0).T[:block] for q in range(n_tp)], axis=0)
    lane = lax.broadcasted_iota(jnp.int32, (rows, 128), 1)
    earlier = lax.broadcasted_iota(jnp.int32, (rows, rows), 1) < lax.broadcasted_iota(jnp.int32, (rows, rows), 0)
    earlier = jnp.where(earlier, 1.0, 0.0).astype(bf)
    taken = jnp.zeros((1, 128), f32)
    places = base
    for k in range(2):
        named = jnp.where(lane.astype(f32) == base[:, k : k + 1], 1.0, 0.0)
        before = jnp.dot(earlier, named.astype(bf), preferred_element_type=f32) + taken
        rank = jnp.sum(before * named, axis=1, keepdims=True)
        taken = taken + jnp.sum(named, axis=0, keepdims=True)
        places = jnp.where(lane == k, base[:, k : k + 1] * cap + rank, places)
    slots_col[...] = places
    slots_row[...] = places.T[:8]
    loads[0].wait()

    width = heads.shape[1]

    def project(x, q):
        return jnp.dot(x, oc[pl.ds(pl.multiple_of(q * width, width), width)], preferred_element_type=f32)

    stream[...] = stream_in[...].astype(f32) + project(heads[...], t)
    for k, d in enumerate((-1, 1)):
        arrived(hall.at[side(d)], asem.at[k])
        ref = hall.at[side(d), pl.ds(k * half, half)]
        remote(ref, ref, sent.at[7], a2sem.at[k], s, side(-d)).start()
    stream[...] += project(hall[side(-1)], side(-1)) + project(hall[side(1)], side(1))
    for k in range(2):
        arrived(hall.at[side(2), pl.ds(k * half, half)], a2sem.at[k])
    total = stream[...] + project(hall[side(2)], side(2))
    stream[...] = total

    part = jnp.sum(total * total, axis=1, keepdims=True)
    ssq[t] = jnp.broadcast_to(part, (rows, 128)).T[:8]
    for d in range(1, n_tp):
        remote(ssq.at[t], ssq.at[t], sent.at[8], qsem.at[d], s, side(d)).start()
    for d in range(1, n_tp):
        arrived(ssq.at[side(-d)], qsem.at[d])
    sums = ssq[0]
    for q in range(1, n_tp):
        sums = sums + ssq[q]
    inv = lax.rsqrt(sums / (feats * n_tp) + EPS)
    inv = jnp.concatenate([inv] * 16, axis=0).T[:, :1]
    normed = (stream[...] * inv * gain[:, pl.ds(pl.multiple_of(t * feats, feats), feats)]).astype(bf)

    own = pltpu.make_async_copy(send.at[s], xbuf.at[t, s], local_sem.at[0])

    def pack(j):
        plane = to_plane(j)
        place = plane * (group * cap) + lax.broadcasted_iota(jnp.int32, (group * cap, rows), 0)
        place = place.astype(f32)
        chosen = (place == slots_row[0:1, :]) | (place == slots_row[1:2, :])
        picked = jnp.dot(jnp.where(chosen, 1.0, 0.0).astype(bf), normed, preferred_element_type=f32)
        send[pl.ds(pl.multiple_of(plane * group, group), group)] = picked.astype(bf).reshape(group, cap, feats)
        return plane

    pack(0)
    own.start()

    def near(i, c):
        dest = z * group + lax.rem(w + i, group)
        remote(send.at[dest], xbuf.at[t, s], sent.at[0], dsem.at[0], dest, t).start()
        return c

    lax.fori_loop(1, group, near, 0)

    def far(j, c):
        plane = pack(j)

        def one(i, c):
            dest = plane * group + lax.rem(w + i, group)
            remote(send.at[dest], xbuf.at[t, s], sent.at[0], dsem.at[j], dest, t).start()
            return c

        return lax.fori_loop(0, group, one, c)

    lax.fori_loop(1, n_z, far, 0)
    for load in loads[1:]:
        load.wait()

    def chunk(q, j):
        return xbuf.at[q, pl.ds(from_plane(j) * group, group)]

    def stage_x(j):
        @pl.when(j == 0)
        def _():
            own.wait()
            arrived(xbuf.at[t, pl.ds(0, group - 1)], dsem.at[0])

        @pl.when(j > 0)
        def _():
            arrived(chunk(t, j), dsem.at[j])

        for k, d in enumerate((1, -1)):
            remote(chunk(t, j), chunk(t, j), sent.at[1], xsem.at[k, j], s, side(d)).start()

    def stage_x2(j):
        arrived(chunk(side(-1), j), xsem.at[0, j])
        arrived(chunk(side(1), j), xsem.at[1, j])
        d = 1 - 2 * lax.rem(j, 2)
        ref = chunk(side(-d), j)
        remote(ref, ref, sent.at[2], x2sem.at[j], s, side(d)).start()

    def stage_up(j):
        arrived(chunk(side(2), j), x2sem.at[j])
        first = pl.multiple_of(from_plane(j) * group, group)
        gate = jnp.zeros((group * cap, units), f32)
        upper = jnp.zeros((group * cap, units), f32)
        for q in range(n_tp):
            x = xbuf[q, pl.ds(first, group)].reshape(group * cap, feats)
            gate = gate + jnp.dot(x, gate_w[q * feats : (q + 1) * feats], preferred_element_type=f32)
            upper = upper + jnp.dot(x, up_w[q * feats : (q + 1) * feats], preferred_element_type=f32)
        act = gate / (1.0 + jnp.exp(-gate)) * upper
        plane = from_plane(j)
        hbuf[t, plane] = act.astype(bf)
        for k, d in enumerate((1, -1)):
            ref = hbuf.at[t, plane]
            remote(ref, ref, sent.at[3], hsem.at[k, j], s, side(d)).start()

    def stage_h2(j):
        plane = from_plane(j)
        arrived(hbuf.at[side(-1), plane], hsem.at[0, j])
        arrived(hbuf.at[side(1), plane], hsem.at[1, j])
        d = 1 - 2 * lax.rem(j, 2)
        ref = hbuf.at[side(-d), plane]
        remote(ref, ref, sent.at[4], h2sem.at[j], s, side(d)).start()

    def stage_down(j):
        plane = from_plane(j)
        arrived(hbuf.at[side(2), plane], h2sem.at[j])
        res = jnp.zeros((group * cap, feats), f32)
        for q in range(n_tp):
            res = res + jnp.dot(hbuf[q, plane], down_w[q * units : (q + 1) * units], preferred_element_type=f32)
        first = pl.multiple_of(plane * group, group)
        rbuf[pl.ds(first, group)] = res.astype(bf).reshape(group, cap, feats)

        @pl.when(j == 0)
        def _():
            pltpu.make_async_copy(rbuf.at[s], back.at[s], local_sem.at[1]).start()

            def one(i, c):
                dest = z * group + lax.rem(w + i, group)
                remote(rbuf.at[dest], back.at[s], sent.at[5], bsem.at[0], dest, t).start()
                return c

            lax.fori_loop(1, group, one, 0)

        @pl.when(j > 0)
        def _():
            def one(i, c):
                dest = plane * group + lax.rem(w + i, group)
                remote(rbuf.at[dest], back.at[s], sent.at[5], bsem.at[j], dest, t).start()
                return c

            lax.fori_loop(0, group, one, 0)

    stages = (stage_x, stage_x2, stage_up, stage_h2, stage_down)

    def step(i, c):
        for lag, stage in enumerate(stages):
            j = i - lag

            @pl.when((j >= 0) & (j < n_z))
            def _():
                stage(j)

        return c

    lax.fori_loop(0, n_z + len(stages) - 1, step, 0)

    pltpu.make_async_copy(rbuf.at[s], back.at[s], local_sem.at[1]).wait()
    arrived(back.at[pl.ds(0, group - 1)], bsem.at[0])

    def home(j, c):
        arrived(back.at[pl.ds(to_plane(j) * group, group)], bsem.at[j])
        return c

    lax.fori_loop(1, n_z, home, 0)

    table = back[...].reshape(n_sp * cap, feats)
    total = stream[...]
    place = lax.broadcasted_iota(jnp.int32, (rows, n_sp * cap), 1).astype(f32)
    for k in range(2):
        chosen = jnp.where(place == slots_col[:, k : k + 1], 1.0, 0.0).astype(bf)
        total = total + slots_col[:, 2 + k : 3 + k] * jnp.dot(chosen, table, preferred_element_type=f32)
    mix[...] = total.astype(bf)
    columns = out.at[:, pl.ds(pl.multiple_of(t * feats, feats), feats)]
    for b in range(n_tp):
        piece = mix.at[pl.ds(b * block, block)]
        if b < n_tp // 2:

            @pl.when(t == b)
            def _():
                pltpu.make_async_copy(piece, columns, local_sem.at[2]).start()

            @pl.when(t != b)
            def _():
                remote(piece, columns, sent.at[9], fsem.at[t], s, b).start()
        else:
            remote(piece, columns, sent.at[9], fsem.at[t], far_s, b).start()
    for q in range(n_tp):
        ref = out.at[:, pl.ds(q * feats, feats)]
        mine = (t == q) & low

        @pl.when(mine)
        def _():
            pltpu.make_async_copy(mix.at[pl.ds(0, block)], ref, local_sem.at[2]).wait()

        @pl.when(jnp.logical_not(mine))
        def _():
            arrived(ref, fsem.at[q])

    left(send.at[pl.ds(0, n_sp - 1)], sent.at[0])
    left(xbuf.at[pl.ds(0, 2)], sent.at[1])
    left(xbuf.at[0], sent.at[2])
    left(hbuf.at[pl.ds(0, 2)], sent.at[3])
    left(hbuf.at[0], sent.at[4])
    left(rbuf.at[pl.ds(0, n_sp - 1)], sent.at[5])
    left(hall.at[pl.ds(0, 2)], sent.at[6])
    left(hall.at[0], sent.at[7])
    left(ssq.at[pl.ds(0, n_tp - 1)], sent.at[8])

    @pl.when(low)
    def _():
        left(mix.at[pl.ds(0, (n_tp - 1) * block)], sent.at[9])

    @pl.when(jnp.logical_not(low))
    def _():
        left(mix, sent.at[9])


def post(heads, out_w, stream_in, gain, meta, gate_w, up_w, down_w, n_sp, n_tp, group, cap):
    rows, feats = stream_in.shape
    units = gate_w.shape[1]
    n_z = n_sp // group
    bf, f32 = jnp.bfloat16, jnp.float32
    dma = pltpu.SemaphoreType.DMA
    vmem, hbm = pl.BlockSpec(memory_space=pltpu.VMEM), pl.BlockSpec(memory_space=pl.ANY)
    return pl.pallas_call(
        functools.partial(post_kernel, n_sp, n_tp, group),
        out_shape=jax.ShapeDtypeStruct((rows // n_tp, feats * n_tp), bf),
        in_specs=[vmem, hbm, vmem, vmem, vmem, hbm, hbm, hbm],
        out_specs=vmem,
        scratch_shapes=[
            pltpu.VMEM((n_tp,) + heads.shape, bf),
            pltpu.VMEM((8, rows), f32),
            pltpu.VMEM((rows, 128), f32),
            pltpu.VMEM(out_w.shape, bf),
            pltpu.VMEM(gate_w.shape, bf),
            pltpu.VMEM(up_w.shape, bf),
            pltpu.VMEM(down_w.shape, bf),
            pltpu.VMEM((rows, feats), f32),
            pltpu.VMEM((n_tp, 8, rows), f32),
            pltpu.VMEM((n_sp, cap, feats), bf),
            pltpu.VMEM((n_tp, n_sp, cap, feats), bf),
            pltpu.VMEM((n_tp, n_z, group * cap, units), bf),
            pltpu.VMEM((n_sp, cap, feats), bf),
            pltpu.VMEM((n_sp, cap, feats), bf),
            pltpu.VMEM((rows, feats), bf),
            dma((10,)), dma((3,)), dma((4,)), dma((2,)), dma((2,)), dma((n_tp,)), dma((n_z,)), dma((2, n_z)),
            dma((n_z,)), dma((2, n_z)), dma((n_z,)), dma((n_z,)), dma((n_tp,)),
        ],
        compiler_params=pltpu.CompilerParams(
            collective_id=1, has_side_effects=True, vmem_limit_bytes=60 * 1024 * 1024),
        name="post",
    )(heads, out_w, stream_in, gain, meta, gate_w, up_w, down_w)


def shards(
    stream_in, queries_one, queries_two, keys_one, keys_two, values, lambdas, head_gain, out_weight,
    norm_gain, expert_ids, route_weight, gate_weight, up_weight, down_weight,
):
    n_sp, n_tp = lax.axis_size("sp"), lax.axis_size("tp")
    meta = jnp.concatenate([expert_ids.astype(jnp.float32), route_weight], 1).T
    meta = jnp.pad(meta, ((0, 8 - meta.shape[0]), (0, 128 - meta.shape[1])))
    heads, stream, meta, out_cols, down_cols = front(
        queries_one, queries_two, keys_one, keys_two, values, stream_in, meta, out_weight, down_weight[0],
        lambdas, head_gain[None], CHIPS + (n_tp, SPLIT),
    )
    return post(
        heads, out_cols, stream, norm_gain[None], meta, gate_weight[0], up_weight[0], down_cols,
        n_sp, n_tp, n_sp // CHIPS[0], CAP,
    )


def solution(mesh):
    return jax.shard_map(
        shards,
        mesh=mesh,
        in_specs=(
            P(("sp", "tp"), None),
            P("sp", "tp"),
            P("sp", "tp"),
            P("sp", "tp"),
            P("sp", "tp"),
            P("sp", "tp"),
            P("tp"),
            P(),
            P("tp", None),
            P(),
            P(("sp", "tp"), None),
            P(("sp", "tp"), None),
            P("sp", None, "tp"),
            P("sp", None, "tp"),
            P("sp", "tp", None),
        ),
        out_specs=P(("sp", "tp"), None),
        check_vma=False,
    )
```

```python
import functools
import math

import jax
import jax.numpy as jnp
from jax import lax
from jax.experimental import pallas as pl
from jax.experimental.pallas import tpu as pltpu
from jax.sharding import PartitionSpec as P

HEAD_DIM = 128
VAL_DIM = 256
EPS = 1e-06
OUT_SCALE = 0.8
SCALE2 = HEAD_DIM ** (-0.5) * math.log2(math.e)
MESH = pl.DeviceIdType.MESH
CHIPS = (8, 4, 2)
SPLIT = 144
CAP = 16
LAST = 14
N_FRONT = 19


def attention_part(dims, queries_one, queries_two, keys_one, keys_two, values, meta_in, out_w, down_w, lam, gain,
                 heads, meta, out_cols, down_cols, kv, q_far, q_all, m_ref, l_ref, acc_ref,
                 sent, local_sem, qsem, msem, osem, wsem, pz, py, py2, ry, ry2, rz, sib):
    n_z, n_y, n_c, n_tp, split = dims
    n_sp = n_z * n_y * n_c
    s, t = lax.axis_index("sp"), lax.axis_index("tp")
    c = lax.rem(s, n_c)
    y = lax.rem(s // n_c, n_y)
    z = s // (n_c * n_y)
    far_s = n_sp - 1 - s
    rows = queries_one.shape[0]
    half = rows // 2
    feats = out_cols.shape[1]
    turn = n_z // 2
    n_keys = n_y // 2 * n_c * rows
    f32, bf = jnp.float32, jnp.bfloat16

    def sp_of(zz, yy, cc):
        return (zz * n_y + yy) * n_c + cc

    def zn(d):
        return lax.rem(z + d + n_z, n_z)

    def yn(d):
        return lax.rem(y + d + n_y, n_y)

    def tn(d):
        return lax.rem(t + d, n_tp)

    def remote(src, dst, a, b, sp, tp):
        return pltpu.make_async_remote_copy(
            src_ref=src, dst_ref=dst, send_sem=a, recv_sem=b, device_id=(sp, tp), device_id_type=MESH)

    def arrived(ref, sem):
        remote(ref, ref, sent.at[0], sem, far_s, t).wait_recv()

    def left(ref, sem):
        remote(ref, ref, sem, qsem.at[0], far_s, t).wait_send()

    mine = kv.at[z, y, c]
    own = [
        pltpu.make_async_copy(keys_one, mine.at[:, pl.ds(0, HEAD_DIM)], local_sem.at[0]),
        pltpu.make_async_copy(keys_two, mine.at[:, pl.ds(HEAD_DIM, HEAD_DIM)], local_sem.at[1]),
        pltpu.make_async_copy(values, mine.at[:, pl.ds(2 * HEAD_DIM, VAL_DIM)], local_sem.at[2]),
    ]
    for copy in own:
        copy.start()

    barrier = pltpu.get_barrier_semaphore()

    def hello(sp, tp):
        pl.semaphore_signal(barrier, inc=1, device_id=(sp, tp), device_id_type=MESH)

    def greet(o, carry):
        hello(lax.rem(s + o, n_sp), t)
        return carry

    lax.fori_loop(1, n_sp, greet, 0)
    for d in range(1, n_tp):
        hello(s, tn(d))
    high = t // (n_tp // 2)

    @pl.when(high == 1)
    def _():
        for q in range(n_tp):
            hello(far_s, q)

    for q in range(n_tp // 2, n_tp):
        hello(far_s, q)
    pl.semaphore_wait(barrier, n_sp - 1 + n_tp - 1 + n_tp // 2 + n_tp * high)
    for copy in own:
        copy.wait()

    def lower(zz, yy):
        return kv.at[zz, yy, c, pl.ds(0, split)]

    def upper(zz, yy):
        return kv.at[zz, yy, c, pl.ds(split, rows - split)]

    def to_z(ref, d, a, sem):
        remote(ref, ref, sent.at[a], sem, sp_of(zn(d), y, c), t).start()

    def to_y(ref, d, a, sem):
        remote(ref, ref, sent.at[a], sem, sp_of(z, yn(d), c), t).start()

    for k, d in enumerate((1, -1)):
        to_z(lower(z, y), d, 0, pz.at[k, 1])
        to_y(upper(z, y), d, 1, ry.at[k])
    for i, queries in enumerate((queries_one, queries_two)):
        remote(queries.at[pl.ds(half, half)], q_far.at[i], sent.at[2], qsem.at[i], far_s, t).start()
    for k, d in enumerate((1, -1)):
        to_z(upper(z, y), d, 3, rz.at[0, k, 1])
        to_y(lower(z, y), d, 4, py.at[0, k])

    sp_home = jnp.where(high == 1, far_s, s)
    for q in range(n_tp):
        at_home = (t == q) & (high == 0)

        @pl.when(at_home)
        def _():
            pltpu.make_async_copy(meta_in, meta.at[t], local_sem.at[4]).start()

        @pl.when(jnp.logical_not(at_home))
        def _():
            remote(meta_in, meta.at[t], sent.at[5], msem.at[t], sp_home, q).start()

    depth, units = out_w.shape[0], down_w.shape[0]
    out_rows = out_cols.at[pl.ds(pl.multiple_of(t * depth, depth), depth)]
    down_rows = down_cols.at[pl.ds(pl.multiple_of(t * units, units), units)]

    def strip(ref, q):
        return ref.at[:, pl.ds(pl.multiple_of(q * feats, feats), feats)]

    for d in range(1, n_tp):
        remote(strip(down_w, tn(d)), down_rows, sent.at[7], wsem.at[d], s, tn(d)).start()
        remote(strip(out_w, tn(d)), out_rows, sent.at[8], osem.at[d], s, tn(d)).start()
    weights = [
        pltpu.make_async_copy(strip(down_w, t), down_rows, local_sem.at[5]),
        pltpu.make_async_copy(strip(out_w, t), out_rows, local_sem.at[6]),
    ]
    for copy in weights:
        copy.start()

    for k, d in enumerate((-1, 1)):
        ref = upper(z, yn(d))
        arrived(ref, ry.at[k])

        @pl.when(c == k)
        def _():
            to_y(ref, -d, 9, ry2.at[0])

        for kk, dd in enumerate((1, -1)):
            to_z(ref, dd, 3, rz.at[1 + k, kk, 1])
    ref = upper(z, yn(2))
    arrived(ref, ry2.at[0])
    for kk, dd in enumerate((1, -1)):
        to_z(ref, dd, 3, rz.at[3, kk, 1])

    m_ref[...] = jnp.full(m_ref.shape, -1e30, f32)
    l_ref[...] = jnp.zeros(l_ref.shape, f32)
    acc_ref[...] = jnp.zeros(acc_ref.shape, f32)

    def plane(j):
        return lax.rem(z + (j + 1) // 2 * (1 - 2 * lax.rem(j, 2)) + n_z, n_z)

    def goes(h, k):
        return (h < turn) | ((h == turn) & (c == k))

    def each_plane(h, f):
        for a in range(2):
            j = jnp.where(h == 0, 0, jnp.minimum(2 * h - 1 + a, n_z - 1))

            @pl.when((a == 0) | ((h >= 1) & (h < turn)))
            def _():
                f(j, plane(j))

    def lower_arrives(h):
        for k, d in enumerate((1, -1)):

            @pl.when(goes(h, k))
            def _():
                zz = zn(-d * h)
                ref = lower(zz, y)
                arrived(ref, pz.at[k, h])

                @pl.when(goes(h + 1, k))
                def _():
                    to_z(ref, d, 0, pz.at[k, h + 1])

                j = jnp.minimum(2 * h - 1 + k, n_z - 1)
                for kk, dd in enumerate((1, -1)):
                    to_y(ref, dd, 4, py.at[j, kk])

    def upper_arrives(h, r):
        yy = lax.rem(y + jnp.where(r == 0, 0, jnp.where(r == 1, n_y - 1, jnp.where(r == 2, 1, 2))), n_y)
        for k, d in enumerate((1, -1)):

            @pl.when(goes(h, k))
            def _():
                ref = upper(zn(-d * h), yy)
                arrived(ref, rz.at[r, k, h])

                @pl.when(goes(h + 1, k))
                def _():
                    to_z(ref, d, 3, rz.at[r, k, h + 1])

    def spread(j, zz):
        arrived(lower(zz, yn(-1)), py.at[j, 0])
        arrived(lower(zz, yn(1)), py.at[j, 1])
        d = 1 - 2 * lax.rem(j, 2)
        to_y(lower(zz, yn(-d)), d, 10, py2.at[j])

    def share(j, zz):
        arrived(lower(zz, yn(2)), py2.at[j])
        ref = kv.at[zz, :, c]
        remote(ref, ref, sent.at[11], sib.at[j], sp_of(z, y, 1 - c), t).start()

    def update(run, zz, part, masked, first_row):
        keys_all = kv[zz, pl.ds(part * (n_y // 2), n_y // 2)].reshape(n_keys, 2 * HEAD_DIM + VAL_DIM)
        v = keys_all[:, 2 * HEAD_DIM :]
        if masked:
            first_key = (zz * 2 + part) * n_keys
            row = first_row + lax.rem(lax.broadcasted_iota(jnp.int32, (rows, n_keys), 0), half)
            keep = first_key + lax.broadcasted_iota(jnp.int32, (rows, n_keys), 1) <= row
        for k in range(2):
            keys = keys_all[:, k * HEAD_DIM : (k + 1) * HEAD_DIM]
            scores = lax.dot_general(q_all[run, k], keys, (((1,), (1,)), ((), ())), preferred_element_type=f32)
            if masked:
                scores = jnp.where(keep, scores, -jnp.inf)
            old = m_ref[run, k]
            new = jnp.maximum(old, jnp.max(scores, axis=1, keepdims=True))
            terms = jnp.exp2((scores - new[:, :1]) * SCALE2)
            fade = jnp.exp2((old - new) * SCALE2)
            lanes = terms[:, :128]
            for i in range(1, n_keys // 128):
                lanes = lanes + terms[:, i * 128 : (i + 1) * 128]
            m_ref[run, k] = new
            l_ref[run, k] = l_ref[run, k] * fade + lanes
            acc_ref[run, k] = acc_ref[run, k] * fade[:, :1] + jnp.dot(terms.astype(bf), v, preferred_element_type=f32)

    def row_of(run):
        return jnp.where(run == 0, s * rows, far_s * rows + half)

    def blocks(run, j):
        return jnp.clip(row_of(run) // n_keys - 2 * plane(j) + 1, 0, 2)

    def attend(n, u):
        at, base = jnp.int32(0), jnp.int32(0)
        count = jnp.int32(0)
        for j in range(n_z):
            count = count + blocks(0, j) + blocks(1, j)
            passed = count <= n
            at = at + jnp.where(passed, 1, 0)
            base = jnp.where(passed, count, base)
        at = jnp.minimum(at, n_z - 1)
        i = n - base
        short = blocks(0, at)
        run = jnp.where(i < short, 0, 1)
        part = i - jnp.where(i < short, 0, short)
        zz = plane(at)

        ready = (n < 2 * n_z + 1) & (u >= 5 * ((at + 1) // 2) + 7)

        @pl.when(ready & (i == 0))
        def _():
            arrived(kv.at[zz, :, 1 - c], sib.at[at])

        here, last = zz * 2 + part, row_of(run) // n_keys

        @pl.when(ready & (here < last))
        def _():
            update(run, zz, part, False, row_of(run))

        @pl.when(ready & (here == last))
        def _():
            update(run, zz, part, True, row_of(run))

        return n + jnp.where(ready, 1, 0)

    spread(jnp.int32(0), z)

    def step(u, done):
        h, sub = u // 5, lax.rem(u, 5)

        @pl.when((sub == 0) & (h <= turn))
        def _():
            lower_arrives(h)

        @pl.when((sub > 0) & (h <= turn))
        def _():
            upper_arrives(h, sub - 1)

        @pl.when((sub == 3) & (h <= turn))
        def _():
            each_plane(h, spread)

        @pl.when((sub == 1) & (h <= turn + 1))
        def _():
            each_plane(h - 1, share)

        @pl.when(u == 6)
        def _():
            for i, queries in enumerate((queries_one, queries_two)):
                arrived(q_far.at[i], qsem.at[i])
                for g in range(2):
                    place = pl.ds(g * half, half)
                    lanes = slice(g * HEAD_DIM, (g + 1) * HEAD_DIM)
                    q_all[0, i, place] = queries[:half, lanes]
                    q_all[1, i, place] = q_far[i, :, lanes]

        return attend(done, u)

    lax.fori_loop(5, 5 * turn + LAST, step, jnp.int32(0))
    for j in range(1, n_z):

        @pl.when(blocks(0, j) + blocks(1, j) == 0)
        def _():
            arrived(kv.at[plane(j), :, 1 - c], sib.at[j])

    for run in range(2):
        mix = [acc_ref[run, k] / jnp.sum(l_ref[run, k], axis=1, keepdims=True) for k in range(2)]
        for g in range(2):
            piece = slice(g * half, (g + 1) * half)
            diff = mix[0][piece] - lam[g] * mix[1][piece]
            ms = jnp.mean(diff * diff, axis=1, keepdims=True)
            res = diff * lax.rsqrt(ms + EPS) * gain[...] * OUT_SCALE
            heads[run * half : (run + 1) * half, g * VAL_DIM : (g + 1) * VAL_DIM] = res.astype(bf)

    for q in range(n_tp):
        at_home = (t == q) & (high == 0)

        @pl.when(at_home)
        def _():
            pltpu.make_async_copy(meta_in, meta.at[q], local_sem.at[4]).wait()

        @pl.when(jnp.logical_not(at_home))
        def _():
            arrived(meta.at[q], msem.at[q])

    for copy in weights:
        copy.wait()
    for d in range(1, n_tp):
        arrived(down_rows, wsem.at[d])
        arrived(out_rows, osem.at[d])
    left(kv.at[pl.ds(0, n_z - 1), 0, 0, pl.ds(0, split)], sent.at[0])
    left(kv.at[0, pl.ds(0, 2), 0, pl.ds(split, rows - split)], sent.at[1])
    left(q_far, sent.at[2])
    left(kv.at[pl.ds(0, n_z - 1), :, 0, pl.ds(split, rows - split)], sent.at[3])
    left(kv.at[:, pl.ds(0, 2), 0, pl.ds(0, split)], sent.at[4])
    left(kv.at[0, 0, 0, pl.ds(split, rows - split)], sent.at[9])
    left(kv.at[:, 0, 0, pl.ds(0, split)], sent.at[10])
    left(kv.at[:, :, 0], sent.at[11])
    for d in range(1, n_tp):
        left(down_rows, sent.at[7])
        left(out_rows, sent.at[8])

    @pl.when(high == 0)
    def _():
        left(meta.at[pl.ds(0, n_tp - 1)], sent.at[5])

    @pl.when(high == 1)
    def _():
        left(meta, sent.at[5])


def experts_part(n_sp, n_tp, group, heads, rows_in, gain, meta, gate_h, up_h,
                out, stream_in, hall, slots_row, slots_col, oc, gate_w, up_w, down_w, stream, ssq, send, xbuf, hbuf, rbuf, back, mix,
                sent, local_sem, wsem, asem, a2sem, qsem, dsem, xsem, x2sem, hsem, h2sem, bsem, fsem, ssem):
    s, t = lax.axis_index("sp"), lax.axis_index("tp")
    n_z = n_sp // group
    z, w = s // group, lax.rem(s, group)
    far_s = n_sp - 1 - s
    cap, feats = send.shape[1], send.shape[2]
    units = gate_w.shape[1]
    rows = heads.shape[0]
    half, block = rows // 2, rows // n_tp
    f32, bf = jnp.float32, jnp.bfloat16

    loads = [
        pltpu.make_async_copy(a, b, wsem.at[i])
        for i, (a, b) in enumerate(((gate_h, gate_w), (up_h, up_w)))
    ]
    for load in loads:
        load.start()

    def side(d):
        return lax.rem(t + d + n_tp, n_tp)

    def offset(j):
        away = (n_z // 2 - j // 2) * jnp.minimum(j, 1)
        return away * (1 - 2 * lax.rem(j, 2))

    def to_plane(j):
        return lax.rem(z + offset(j) + n_z, n_z)

    def from_plane(j):
        return lax.rem(z - offset(j) + n_z, n_z)

    def remote(src, dst, a, b, sp, tp):
        return pltpu.make_async_remote_copy(
            src_ref=src, dst_ref=dst, send_sem=a, recv_sem=b, device_id=(sp, tp), device_id_type=MESH)

    def arrived(ref, sem):
        remote(ref, ref, sent.at[0], sem, s, side(1)).wait_recv()

    def left(ref, sem):
        remote(ref, ref, sem, dsem.at[0], s, side(1)).wait_send()

    low = t < n_tp // 2

    for k, d in enumerate((1, -1)):
        remote(heads, hall.at[t], sent.at[6], asem.at[k], s, side(d)).start()

    sp_home = jnp.where(low, s, far_s)
    slab = stream_in.at[pl.ds(pl.multiple_of(t * block, block), block)]
    for q in range(n_tp):
        piece = rows_in.at[:, pl.ds(q * feats, feats)]
        at_home = (t == q) & low

        @pl.when(at_home)
        def _():
            pltpu.make_async_copy(piece, slab, local_sem.at[3]).start()

        @pl.when(jnp.logical_not(at_home))
        def _():
            remote(piece, slab, sent.at[10], ssem.at[t], sp_home, q).start()

    base = jnp.concatenate([jnp.concatenate([meta[q]] * 16, axis=0).T[:block] for q in range(n_tp)], axis=0)
    lane = lax.broadcasted_iota(jnp.int32, (rows, 128), 1)
    earlier = lax.broadcasted_iota(jnp.int32, (rows, rows), 1) < lax.broadcasted_iota(jnp.int32, (rows, rows), 0)
    earlier = jnp.where(earlier, 1.0, 0.0).astype(bf)
    taken = jnp.zeros((1, 128), f32)
    places = base
    for k in range(2):
        named = jnp.where(lane.astype(f32) == base[:, k : k + 1], 1.0, 0.0)
        before = jnp.dot(earlier, named.astype(bf), preferred_element_type=f32) + taken
        rank = jnp.sum(before * named, axis=1, keepdims=True)
        taken = taken + jnp.sum(named, axis=0, keepdims=True)
        places = jnp.where(lane == k, base[:, k : k + 1] * cap + rank, places)
    slots_col[...] = places
    slots_row[...] = places.T[:8]

    width = heads.shape[1]

    def project(x, q):
        return jnp.dot(x, oc[pl.ds(pl.multiple_of(q * width, width), width)], preferred_element_type=f32)

    stream[...] = project(heads[...], t)
    for k, d in enumerate((-1, 1)):
        arrived(hall.at[side(d)], asem.at[k])
        ref = hall.at[side(d), pl.ds(k * half, half)]
        remote(ref, ref, sent.at[7], a2sem.at[k], s, side(-d)).start()
    stream[...] += project(hall[side(-1)], side(-1)) + project(hall[side(1)], side(1))
    for k in range(2):
        arrived(hall.at[side(2), pl.ds(k * half, half)], a2sem.at[k])
    for q in range(n_tp):
        ref = stream_in.at[pl.ds(q * block, block)]
        at_home = (t == q) & low

        @pl.when(at_home)
        def _():
            pltpu.make_async_copy(rows_in.at[:, pl.ds(q * feats, feats)], ref, local_sem.at[3]).wait()

        @pl.when(jnp.logical_not(at_home))
        def _():
            arrived(ref, ssem.at[q])

    total = stream[...] + project(hall[side(2)], side(2)) + stream_in[...].astype(f32)
    stream[...] = total

    part = jnp.sum(total * total, axis=1, keepdims=True)
    ssq[t] = jnp.broadcast_to(part, (rows, 128)).T[:8]
    for d in range(1, n_tp):
        remote(ssq.at[t], ssq.at[t], sent.at[8], qsem.at[d], s, side(d)).start()
    for d in range(1, n_tp):
        arrived(ssq.at[side(-d)], qsem.at[d])
    sums = ssq[0]
    for q in range(1, n_tp):
        sums = sums + ssq[q]
    inv = lax.rsqrt(sums / (feats * n_tp) + EPS)
    inv = jnp.concatenate([inv] * 16, axis=0).T[:, :1]
    normed = (stream[...] * inv * gain[:, pl.ds(pl.multiple_of(t * feats, feats), feats)]).astype(bf)

    own = pltpu.make_async_copy(send.at[s], xbuf.at[t, s], local_sem.at[0])

    def pack(j):
        plane = to_plane(j)
        place = plane * (group * cap) + lax.broadcasted_iota(jnp.int32, (group * cap, rows), 0)
        place = place.astype(f32)
        chosen = (place == slots_row[0:1, :]) | (place == slots_row[1:2, :])
        picked = jnp.dot(jnp.where(chosen, 1.0, 0.0).astype(bf), normed, preferred_element_type=f32)
        send[pl.ds(pl.multiple_of(plane * group, group), group)] = picked.astype(bf).reshape(group, cap, feats)
        return plane

    pack(0)
    own.start()

    def near(i, c):
        dest = z * group + lax.rem(w + i, group)
        remote(send.at[dest], xbuf.at[t, s], sent.at[0], dsem.at[0], dest, t).start()
        return c

    lax.fori_loop(1, group, near, 0)

    def far(j, c):
        plane = pack(j)

        def one(i, c):
            dest = plane * group + lax.rem(w + i, group)
            remote(send.at[dest], xbuf.at[t, s], sent.at[0], dsem.at[j], dest, t).start()
            return c

        return lax.fori_loop(0, group, one, c)

    lax.fori_loop(1, n_z, far, 0)
    for load in loads:
        load.wait()

    def chunk(q, j):
        return xbuf.at[q, pl.ds(from_plane(j) * group, group)]

    def stage_x(j):
        @pl.when(j == 0)
        def _():
            own.wait()
            arrived(xbuf.at[t, pl.ds(0, group - 1)], dsem.at[0])

        @pl.when(j > 0)
        def _():
            arrived(chunk(t, j), dsem.at[j])

        for k, d in enumerate((1, -1)):
            remote(chunk(t, j), chunk(t, j), sent.at[1], xsem.at[k, j], s, side(d)).start()

    def stage_x2(j):
        arrived(chunk(side(-1), j), xsem.at[0, j])
        arrived(chunk(side(1), j), xsem.at[1, j])
        d = 1 - 2 * lax.rem(j, 2)
        ref = chunk(side(-d), j)
        remote(ref, ref, sent.at[2], x2sem.at[j], s, side(d)).start()

    def stage_up(j):
        arrived(chunk(side(2), j), x2sem.at[j])
        first = pl.multiple_of(from_plane(j) * group, group)
        gate = jnp.zeros((group * cap, units), f32)
        upper = jnp.zeros((group * cap, units), f32)
        for q in range(n_tp):
            x = xbuf[q, pl.ds(first, group)].reshape(group * cap, feats)
            gate = gate + jnp.dot(x, gate_w[q * feats : (q + 1) * feats], preferred_element_type=f32)
            upper = upper + jnp.dot(x, up_w[q * feats : (q + 1) * feats], preferred_element_type=f32)
        act = gate / (1.0 + jnp.exp(-gate)) * upper
        plane = from_plane(j)
        hbuf[t, plane] = act.astype(bf)
        for k, d in enumerate((1, -1)):
            ref = hbuf.at[t, plane]
            remote(ref, ref, sent.at[3], hsem.at[k, j], s, side(d)).start()

    def stage_h2(j):
        plane = from_plane(j)
        arrived(hbuf.at[side(-1), plane], hsem.at[0, j])
        arrived(hbuf.at[side(1), plane], hsem.at[1, j])
        d = 1 - 2 * lax.rem(j, 2)
        ref = hbuf.at[side(-d), plane]
        remote(ref, ref, sent.at[4], h2sem.at[j], s, side(d)).start()

    def stage_down(j):
        plane = from_plane(j)
        arrived(hbuf.at[side(2), plane], h2sem.at[j])
        res = jnp.zeros((group * cap, feats), f32)
        for q in range(n_tp):
            res = res + jnp.dot(hbuf[q, plane], down_w[q * units : (q + 1) * units], preferred_element_type=f32)
        first = pl.multiple_of(plane * group, group)
        rbuf[pl.ds(first, group)] = res.astype(bf).reshape(group, cap, feats)

        @pl.when(j == 0)
        def _():
            pltpu.make_async_copy(rbuf.at[s], back.at[s], local_sem.at[1]).start()

            def one(i, c):
                dest = z * group + lax.rem(w + i, group)
                remote(rbuf.at[dest], back.at[s], sent.at[5], bsem.at[0], dest, t).start()
                return c

            lax.fori_loop(1, group, one, 0)

        @pl.when(j > 0)
        def _():
            def one(i, c):
                dest = plane * group + lax.rem(w + i, group)
                remote(rbuf.at[dest], back.at[s], sent.at[5], bsem.at[j], dest, t).start()
                return c

            lax.fori_loop(0, group, one, 0)

    stages = (stage_x, stage_x2, stage_up, stage_h2, stage_down)

    def step(i, c):
        for lag, stage in enumerate(stages):
            j = i - lag

            @pl.when((j >= 0) & (j < n_z))
            def _():
                stage(j)

        return c

    lax.fori_loop(0, n_z + len(stages) - 1, step, 0)

    pltpu.make_async_copy(rbuf.at[s], back.at[s], local_sem.at[1]).wait()
    arrived(back.at[pl.ds(0, group - 1)], bsem.at[0])

    def home(j, c):
        arrived(back.at[pl.ds(to_plane(j) * group, group)], bsem.at[j])
        return c

    lax.fori_loop(1, n_z, home, 0)

    table = back[...].reshape(n_sp * cap, feats)
    total = stream[...]
    place = lax.broadcasted_iota(jnp.int32, (rows, n_sp * cap), 1).astype(f32)
    for k in range(2):
        chosen = jnp.where(place == slots_col[:, k : k + 1], 1.0, 0.0).astype(bf)
        total = total + slots_col[:, 2 + k : 3 + k] * jnp.dot(chosen, table, preferred_element_type=f32)
    mix[...] = total.astype(bf)
    columns = out.at[:, pl.ds(pl.multiple_of(t * feats, feats), feats)]
    for b in range(n_tp):
        piece = mix.at[pl.ds(b * block, block)]
        if b < n_tp // 2:

            @pl.when(t == b)
            def _():
                pltpu.make_async_copy(piece, columns, local_sem.at[2]).start()

            @pl.when(t != b)
            def _():
                remote(piece, columns, sent.at[9], fsem.at[t], s, b).start()
        else:
            remote(piece, columns, sent.at[9], fsem.at[t], far_s, b).start()
    for q in range(n_tp):
        ref = out.at[:, pl.ds(q * feats, feats)]
        mine = (t == q) & low

        @pl.when(mine)
        def _():
            pltpu.make_async_copy(mix.at[pl.ds(0, block)], ref, local_sem.at[2]).wait()

        @pl.when(jnp.logical_not(mine))
        def _():
            arrived(ref, fsem.at[q])

    left(send.at[pl.ds(0, n_sp - 1)], sent.at[0])
    left(xbuf.at[pl.ds(0, 2)], sent.at[1])
    left(xbuf.at[0], sent.at[2])
    left(hbuf.at[pl.ds(0, 2)], sent.at[3])
    left(hbuf.at[0], sent.at[4])
    left(rbuf.at[pl.ds(0, n_sp - 1)], sent.at[5])
    left(hall.at[pl.ds(0, 2)], sent.at[6])
    left(hall.at[0], sent.at[7])
    left(ssq.at[pl.ds(0, n_tp - 1)], sent.at[8])

    @pl.when(low)
    def _():
        left(mix.at[pl.ds(0, (n_tp - 1) * block)], sent.at[9])
        left(mix.at[pl.ds(0, (n_tp - 1) * block)], sent.at[10])

    @pl.when(jnp.logical_not(low))
    def _():
        left(mix, sent.at[9])
        left(mix, sent.at[10])


def layer_kernel(dims, queries_one, queries_two, keys_one, keys_two, values, meta_in, out_w, down_w, lam, head_gain,
                 rows_in, norm_gain, gate_h, up_h, out, heads, meta, oc, down, *rest):
    attention_part(
        dims, queries_one, queries_two, keys_one, keys_two, values, meta_in, out_w, down_w, lam, head_gain,
        heads, meta, oc, down, *rest[:N_FRONT],
    )
    n_z, n_y, n_c, n_tp, _ = dims
    stream_in, hall, slots_row, slots_col, gate_w, up_w, *tail = rest[N_FRONT:]
    experts_part(
        n_z * n_y * n_c, n_tp, n_y * n_c, heads, rows_in, norm_gain, meta, gate_h, up_h,
        out, stream_in, hall, slots_row, slots_col, oc, gate_w, up_w, down, *tail,
    )


def layer(queries_one, queries_two, keys_one, keys_two, values, meta, out_w, down_w, lam, head_gain,
          rows_in, norm_gain, gate_w, up_w, dims):
    n_z, n_y, n_c, n_tp, split = dims
    n_sp, group = n_z * n_y * n_c, n_y * n_c
    rows = queries_one.shape[0]
    feats = out_w.shape[1] // n_tp
    units, cap = gate_w.shape[1], CAP
    turn = n_z // 2
    bf, f32 = jnp.bfloat16, jnp.float32
    dma = pltpu.SemaphoreType.DMA
    vmem, hbm = pl.BlockSpec(memory_space=pltpu.VMEM), pl.BlockSpec(memory_space=pl.ANY)
    smem = pl.BlockSpec(memory_space=pltpu.SMEM)
    first = [
        pltpu.VMEM((n_z, n_y, n_c, rows, 2 * HEAD_DIM + VAL_DIM), bf),
        pltpu.VMEM((2, rows // 2, 2 * HEAD_DIM), bf),
        pltpu.VMEM((2, 2, rows, HEAD_DIM), bf),
        pltpu.VMEM((2, 2, rows, 128), f32),
        pltpu.VMEM((2, 2, rows, 128), f32),
        pltpu.VMEM((2, 2, rows, VAL_DIM), f32),
        dma((12,)), dma((7,)), dma((2,)), dma((n_tp,)), dma((n_tp,)), dma((n_tp,)),
        dma((2, turn + 1)), dma((n_z, 2)), dma((n_z,)), dma((2,)), dma((1,)), dma((4, 2, turn + 1)), dma((n_z,)),
    ]
    assert len(first) == N_FRONT
    second = [
        pltpu.VMEM((rows, feats), bf),
        pltpu.VMEM((n_tp, rows, 2 * VAL_DIM), bf),
        pltpu.VMEM((8, rows), f32),
        pltpu.VMEM((rows, 128), f32),
        pltpu.VMEM(gate_w.shape, bf),
        pltpu.VMEM(up_w.shape, bf),
        pltpu.VMEM((rows, feats), f32),
        pltpu.VMEM((n_tp, 8, rows), f32),
        pltpu.VMEM((n_sp, cap, feats), bf),
        pltpu.VMEM((n_tp, n_sp, cap, feats), bf),
        pltpu.VMEM((n_tp, n_z, group * cap, units), bf),
        pltpu.VMEM((n_sp, cap, feats), bf),
        pltpu.VMEM((n_sp, cap, feats), bf),
        pltpu.VMEM((rows, feats), bf),
        dma((11,)), dma((4,)), dma((4,)), dma((2,)), dma((2,)), dma((n_tp,)), dma((n_z,)), dma((2, n_z)),
        dma((n_z,)), dma((2, n_z)), dma((n_z,)), dma((n_z,)), dma((n_tp,)), dma((n_tp,)),
    ]
    return pl.pallas_call(
        functools.partial(layer_kernel, dims),
        out_shape=jax.ShapeDtypeStruct((rows // n_tp, feats * n_tp), bf),
        in_specs=[vmem, vmem, hbm, hbm, hbm, vmem, hbm, hbm, smem, vmem, vmem, vmem, hbm, hbm],
        out_specs=vmem,
        scratch_shapes=[
            pltpu.VMEM((rows, 2 * VAL_DIM), bf),
            pltpu.VMEM((n_tp,) + meta.shape, f32),
            pltpu.VMEM((n_tp * out_w.shape[0], feats), bf),
            pltpu.VMEM((n_tp * down_w.shape[0], feats), bf),
        ]
        + first
        + second,
        compiler_params=pltpu.CompilerParams(
            collective_id=0, has_side_effects=True, vmem_limit_bytes=60 * 1024 * 1024),
        name="layer",
    )(queries_one, queries_two, keys_one, keys_two, values, meta, out_w, down_w, lam, head_gain,
      rows_in, norm_gain, gate_w, up_w)


def shards(
    stream_in, queries_one, queries_two, keys_one, keys_two, values, lambdas, head_gain, out_weight,
    norm_gain, expert_ids, route_weight, gate_weight, up_weight, down_weight,
):
    meta = jnp.concatenate([expert_ids.astype(jnp.float32), route_weight], 1).T
    meta = jnp.pad(meta, ((0, 8 - meta.shape[0]), (0, 128 - meta.shape[1])))
    return layer(
        queries_one, queries_two, keys_one, keys_two, values, meta, out_weight, down_weight[0], lambdas, head_gain[None],
        stream_in, norm_gain[None], gate_weight[0], up_weight[0], CHIPS + (lax.axis_size("tp"), SPLIT),
    )


def solution(mesh):
    return jax.shard_map(
        shards,
        mesh=mesh,
        in_specs=(
            P(("sp", "tp"), None),
            P("sp", "tp"),
            P("sp", "tp"),
            P("sp", "tp"),
            P("sp", "tp"),
            P("sp", "tp"),
            P("tp"),
            P(),
            P("tp", None),
            P(),
            P(("sp", "tp"), None),
            P(("sp", "tp"), None),
            P("sp", None, "tp"),
            P("sp", None, "tp"),
            P("sp", "tp", None),
        ),
        out_specs=P(("sp", "tp"), None),
        check_vma=False,
    )
```

```python
import functools
import math

import jax
import jax.numpy as jnp
from jax import lax
from jax.experimental import pallas as pl
from jax.experimental.pallas import tpu as pltpu
from jax.sharding import PartitionSpec as P

HEAD_DIM = 128
VAL_DIM = 256
EPS = 1e-06
OUT_SCALE = 0.8
SCALE2 = HEAD_DIM ** (-0.5) * math.log2(math.e)
MESH = pl.DeviceIdType.MESH
CHIPS = (8, 4, 2)
SPLIT = 144
CAP = 16
LAST = 14
N_FRONT = 19


def attention_part(dims, late, queries_one, queries_two, keys_one, keys_two, values, meta_in, out_w, down_w, lam, gain,
                 heads, meta, out_cols, down_cols, kv, q_far, q_all, m_ref, l_ref, acc_ref,
                 sent, local_sem, qsem, msem, osem, wsem, pz, py, py2, ry, ry2, rz, sib):
    n_z, n_y, n_c, n_tp, split = dims
    n_sp = n_z * n_y * n_c
    s, t = lax.axis_index("sp"), lax.axis_index("tp")
    c = lax.rem(s, n_c)
    y = lax.rem(s // n_c, n_y)
    z = s // (n_c * n_y)
    far_s = n_sp - 1 - s
    rows = queries_one.shape[0]
    half = rows // 2
    feats = out_cols.shape[1]
    turn = n_z // 2
    n_keys = n_y // 2 * n_c * rows
    f32, bf = jnp.float32, jnp.bfloat16

    def sp_of(zz, yy, cc):
        return (zz * n_y + yy) * n_c + cc

    def zn(d):
        return lax.rem(z + d + n_z, n_z)

    def yn(d):
        return lax.rem(y + d + n_y, n_y)

    def tn(d):
        return lax.rem(t + d, n_tp)

    def remote(src, dst, a, b, sp, tp):
        return pltpu.make_async_remote_copy(
            src_ref=src, dst_ref=dst, send_sem=a, recv_sem=b, device_id=(sp, tp), device_id_type=MESH)

    def arrived(ref, sem):
        remote(ref, ref, sent.at[0], sem, far_s, t).wait_recv()

    def left(ref, sem):
        remote(ref, ref, sem, qsem.at[0], far_s, t).wait_send()

    mine = kv.at[z, y, c]
    own = [
        pltpu.make_async_copy(keys_one, mine.at[:, pl.ds(0, HEAD_DIM)], local_sem.at[0]),
        pltpu.make_async_copy(keys_two, mine.at[:, pl.ds(HEAD_DIM, HEAD_DIM)], local_sem.at[1]),
        pltpu.make_async_copy(values, mine.at[:, pl.ds(2 * HEAD_DIM, VAL_DIM)], local_sem.at[2]),
    ]
    for copy in own:
        copy.start()

    barrier = pltpu.get_barrier_semaphore()

    def hello(sp, tp):
        pl.semaphore_signal(barrier, inc=1, device_id=(sp, tp), device_id_type=MESH)

    def greet(o, carry):
        hello(lax.rem(s + o, n_sp), t)
        return carry

    lax.fori_loop(1, n_sp, greet, 0)
    for d in range(1, n_tp):
        hello(s, tn(d))
    high = t // (n_tp // 2)

    @pl.when(high == 1)
    def _():
        for q in range(n_tp):
            hello(far_s, q)

    for q in range(n_tp // 2, n_tp):
        hello(far_s, q)
    pl.semaphore_wait(barrier, n_sp - 1 + n_tp - 1 + n_tp // 2 + n_tp * high)
    for copy in own:
        copy.wait()

    def lower(zz, yy):
        return kv.at[zz, yy, c, pl.ds(0, split)]

    def upper(zz, yy):
        return kv.at[zz, yy, c, pl.ds(split, rows - split)]

    def to_z(ref, d, a, sem):
        remote(ref, ref, sent.at[a], sem, sp_of(zn(d), y, c), t).start()

    def to_y(ref, d, a, sem):
        remote(ref, ref, sent.at[a], sem, sp_of(z, yn(d), c), t).start()

    for k, d in enumerate((1, -1)):
        to_z(lower(z, y), d, 0, pz.at[k, 1])
        to_y(upper(z, y), d, 1, ry.at[k])
    for i, queries in enumerate((queries_one, queries_two)):
        remote(queries.at[pl.ds(half, half)], q_far.at[i], sent.at[2], qsem.at[i], far_s, t).start()
    for k, d in enumerate((1, -1)):
        to_z(upper(z, y), d, 3, rz.at[0, k, 1])
        to_y(lower(z, y), d, 4, py.at[0, k])

    sp_home = jnp.where(high == 1, far_s, s)
    for q in range(n_tp):
        at_home = (t == q) & (high == 0)

        @pl.when(at_home)
        def _():
            pltpu.make_async_copy(meta_in, meta.at[t], local_sem.at[4]).start()

        @pl.when(jnp.logical_not(at_home))
        def _():
            remote(meta_in, meta.at[t], sent.at[5], msem.at[t], sp_home, q).start()

    depth, units = out_w.shape[0], down_w.shape[0]
    out_rows = out_cols.at[pl.ds(pl.multiple_of(t * depth, depth), depth)]
    down_rows = down_cols.at[pl.ds(pl.multiple_of(t * units, units), units)]

    def strip(ref, q):
        return ref.at[:, pl.ds(pl.multiple_of(q * feats, feats), feats)]

    for d in range(1, n_tp):
        remote(strip(down_w, tn(d)), down_rows, sent.at[7], wsem.at[d], s, tn(d)).start()
        remote(strip(out_w, tn(d)), out_rows, sent.at[8], osem.at[d], s, tn(d)).start()
    weights = [
        pltpu.make_async_copy(strip(down_w, t), down_rows, local_sem.at[5]),
        pltpu.make_async_copy(strip(out_w, t), out_rows, local_sem.at[6]),
    ]
    for copy in weights:
        copy.start()

    for k, d in enumerate((-1, 1)):
        ref = upper(z, yn(d))
        arrived(ref, ry.at[k])

        @pl.when(c == k)
        def _():
            to_y(ref, -d, 9, ry2.at[0])

        for kk, dd in enumerate((1, -1)):
            to_z(ref, dd, 3, rz.at[1 + k, kk, 1])
    ref = upper(z, yn(2))
    arrived(ref, ry2.at[0])
    for kk, dd in enumerate((1, -1)):
        to_z(ref, dd, 3, rz.at[3, kk, 1])

    m_ref[...] = jnp.full(m_ref.shape, -1e30, f32)
    l_ref[...] = jnp.zeros(l_ref.shape, f32)
    acc_ref[...] = jnp.zeros(acc_ref.shape, f32)

    def plane(j):
        return lax.rem(z + (j + 1) // 2 * (1 - 2 * lax.rem(j, 2)) + n_z, n_z)

    def goes(h, k):
        return (h < turn) | ((h == turn) & (c == k))

    def each_plane(h, f):
        for a in range(2):
            j = jnp.where(h == 0, 0, jnp.minimum(2 * h - 1 + a, n_z - 1))

            @pl.when((a == 0) | ((h >= 1) & (h < turn)))
            def _():
                f(j, plane(j))

    def lower_arrives(h):
        for k, d in enumerate((1, -1)):

            @pl.when(goes(h, k))
            def _():
                zz = zn(-d * h)
                ref = lower(zz, y)
                arrived(ref, pz.at[k, h])

                @pl.when(goes(h + 1, k))
                def _():
                    to_z(ref, d, 0, pz.at[k, h + 1])

                j = jnp.minimum(2 * h - 1 + k, n_z - 1)
                for kk, dd in enumerate((1, -1)):
                    to_y(ref, dd, 4, py.at[j, kk])

    def upper_arrives(h, r):
        yy = lax.rem(y + jnp.where(r == 0, 0, jnp.where(r == 1, n_y - 1, jnp.where(r == 2, 1, 2))), n_y)
        for k, d in enumerate((1, -1)):

            @pl.when(goes(h, k))
            def _():
                ref = upper(zn(-d * h), yy)
                arrived(ref, rz.at[r, k, h])

                @pl.when(goes(h + 1, k))
                def _():
                    to_z(ref, d, 3, rz.at[r, k, h + 1])

    def spread(j, zz):
        arrived(lower(zz, yn(-1)), py.at[j, 0])
        arrived(lower(zz, yn(1)), py.at[j, 1])
        d = 1 - 2 * lax.rem(j, 2)
        to_y(lower(zz, yn(-d)), d, 10, py2.at[j])

    def share(j, zz):
        arrived(lower(zz, yn(2)), py2.at[j])
        ref = kv.at[zz, :, c]
        remote(ref, ref, sent.at[11], sib.at[j], sp_of(z, y, 1 - c), t).start()

    def update(run, zz, part, masked, first_row):
        keys_all = kv[zz, pl.ds(part * (n_y // 2), n_y // 2)].reshape(n_keys, 2 * HEAD_DIM + VAL_DIM)
        v = keys_all[:, 2 * HEAD_DIM :]
        if masked:
            first_key = (zz * 2 + part) * n_keys
            row = first_row + lax.rem(lax.broadcasted_iota(jnp.int32, (rows, n_keys), 0), half)
            keep = first_key + lax.broadcasted_iota(jnp.int32, (rows, n_keys), 1) <= row
        for k in range(2):
            keys = keys_all[:, k * HEAD_DIM : (k + 1) * HEAD_DIM]
            scores = lax.dot_general(q_all[run, k], keys, (((1,), (1,)), ((), ())), preferred_element_type=f32)
            if masked:
                scores = jnp.where(keep, scores, -jnp.inf)
            old = m_ref[run, k]
            new = jnp.maximum(old, jnp.max(scores, axis=1, keepdims=True))
            terms = jnp.exp2((scores - new[:, :1]) * SCALE2)
            fade = jnp.exp2((old - new) * SCALE2)
            lanes = terms[:, :128]
            for i in range(1, n_keys // 128):
                lanes = lanes + terms[:, i * 128 : (i + 1) * 128]
            m_ref[run, k] = new
            l_ref[run, k] = l_ref[run, k] * fade + lanes
            acc_ref[run, k] = acc_ref[run, k] * fade[:, :1] + jnp.dot(terms.astype(bf), v, preferred_element_type=f32)

    def row_of(run):
        return jnp.where(run == 0, s * rows, far_s * rows + half)

    def blocks(run, j):
        return jnp.clip(row_of(run) // n_keys - 2 * plane(j) + 1, 0, 2)

    def attend(n, u):
        at, base = jnp.int32(0), jnp.int32(0)
        count = jnp.int32(0)
        for j in range(n_z):
            count = count + blocks(0, j) + blocks(1, j)
            passed = count <= n
            at = at + jnp.where(passed, 1, 0)
            base = jnp.where(passed, count, base)
        at = jnp.minimum(at, n_z - 1)
        i = n - base
        short = blocks(0, at)
        run = jnp.where(i < short, 0, 1)
        part = i - jnp.where(i < short, 0, short)
        zz = plane(at)

        ready = (n < 2 * n_z + 1) & (u >= 5 * ((at + 1) // 2) + 7)

        @pl.when(ready & (i == 0))
        def _():
            arrived(kv.at[zz, :, 1 - c], sib.at[at])

        here, last = zz * 2 + part, row_of(run) // n_keys

        @pl.when(ready & (here < last))
        def _():
            update(run, zz, part, False, row_of(run))

        @pl.when(ready & (here == last))
        def _():
            update(run, zz, part, True, row_of(run))

        return n + jnp.where(ready, 1, 0)

    spread(jnp.int32(0), z)

    def step(u, done):
        h, sub = u // 5, lax.rem(u, 5)

        @pl.when((sub == 0) & (h <= turn))
        def _():
            lower_arrives(h)

        @pl.when((sub > 0) & (h <= turn))
        def _():
            upper_arrives(h, sub - 1)

        @pl.when((sub == 3) & (h <= turn))
        def _():
            each_plane(h, spread)

        @pl.when((sub == 1) & (h <= turn + 1))
        def _():
            each_plane(h - 1, share)

        @pl.when(u == 6)
        def _():
            for i, queries in enumerate((queries_one, queries_two)):
                arrived(q_far.at[i], qsem.at[i])
                for g in range(2):
                    place = pl.ds(g * half, half)
                    lanes = slice(g * HEAD_DIM, (g + 1) * HEAD_DIM)
                    q_all[0, i, place] = queries[:half, lanes]
                    q_all[1, i, place] = q_far[i, :, lanes]

        @pl.when(u == 5 * turn + 6)
        def _():
            late()

        return attend(done, u)

    lax.fori_loop(5, 5 * turn + LAST, step, jnp.int32(0))
    for j in range(1, n_z):

        @pl.when(blocks(0, j) + blocks(1, j) == 0)
        def _():
            arrived(kv.at[plane(j), :, 1 - c], sib.at[j])

    for run in range(2):
        mix = [acc_ref[run, k] / jnp.sum(l_ref[run, k], axis=1, keepdims=True) for k in range(2)]
        for g in range(2):
            piece = slice(g * half, (g + 1) * half)
            diff = mix[0][piece] - lam[g] * mix[1][piece]
            ms = jnp.mean(diff * diff, axis=1, keepdims=True)
            res = diff * lax.rsqrt(ms + EPS) * gain[...] * OUT_SCALE
            heads[run * half : (run + 1) * half, g * VAL_DIM : (g + 1) * VAL_DIM] = res.astype(bf)

    for q in range(n_tp):
        at_home = (t == q) & (high == 0)

        @pl.when(at_home)
        def _():
            pltpu.make_async_copy(meta_in, meta.at[q], local_sem.at[4]).wait()

        @pl.when(jnp.logical_not(at_home))
        def _():
            arrived(meta.at[q], msem.at[q])

    for copy in weights:
        copy.wait()
    for d in range(1, n_tp):
        arrived(down_rows, wsem.at[d])
        arrived(out_rows, osem.at[d])
    left(kv.at[pl.ds(0, n_z - 1), 0, 0, pl.ds(0, split)], sent.at[0])
    left(kv.at[0, pl.ds(0, 2), 0, pl.ds(split, rows - split)], sent.at[1])
    left(q_far, sent.at[2])
    left(kv.at[pl.ds(0, n_z - 1), :, 0, pl.ds(split, rows - split)], sent.at[3])
    left(kv.at[:, pl.ds(0, 2), 0, pl.ds(0, split)], sent.at[4])
    left(kv.at[0, 0, 0, pl.ds(split, rows - split)], sent.at[9])
    left(kv.at[:, 0, 0, pl.ds(0, split)], sent.at[10])
    left(kv.at[:, :, 0], sent.at[11])
    for d in range(1, n_tp):
        left(down_rows, sent.at[7])
        left(out_rows, sent.at[8])

    @pl.when(high == 0)
    def _():
        left(meta.at[pl.ds(0, n_tp - 1)], sent.at[5])

    @pl.when(high == 1)
    def _():
        left(meta, sent.at[5])


def experts_part(n_sp, n_tp, group, heads, rows_in, gain, meta, gate_h, up_h,
                out, stream_in, hall, slots_row, slots_col, oc, gate_w, up_w, down_w, stream, ssq, send, xbuf, hbuf, rbuf, back, mix,
                sent, local_sem, wsem, asem, a2sem, qsem, dsem, xsem, x2sem, hsem, h2sem, bsem, fsem, ssem):
    s, t = lax.axis_index("sp"), lax.axis_index("tp")
    n_z = n_sp // group
    z, w = s // group, lax.rem(s, group)
    far_s = n_sp - 1 - s
    cap, feats = send.shape[1], send.shape[2]
    units = gate_w.shape[1]
    rows = heads.shape[0]
    half, block = rows // 2, rows // n_tp
    f32, bf = jnp.float32, jnp.bfloat16

    loads = [
        pltpu.make_async_copy(a, b, wsem.at[i])
        for i, (a, b) in enumerate(((gate_h, gate_w), (up_h, up_w)))
    ]
    for load in loads:
        load.start()

    def side(d):
        return lax.rem(t + d + n_tp, n_tp)

    def offset(j):
        away = (n_z // 2 - j // 2) * jnp.minimum(j, 1)
        return away * (1 - 2 * lax.rem(j, 2))

    def to_plane(j):
        return lax.rem(z + offset(j) + n_z, n_z)

    def from_plane(j):
        return lax.rem(z - offset(j) + n_z, n_z)

    def remote(src, dst, a, b, sp, tp):
        return pltpu.make_async_remote_copy(
            src_ref=src, dst_ref=dst, send_sem=a, recv_sem=b, device_id=(sp, tp), device_id_type=MESH)

    def arrived(ref, sem):
        remote(ref, ref, sent.at[0], sem, s, side(1)).wait_recv()

    def left(ref, sem):
        remote(ref, ref, sem, dsem.at[0], s, side(1)).wait_send()

    low = t < n_tp // 2

    for k, d in enumerate((1, -1)):
        remote(heads, hall.at[t], sent.at[6], asem.at[k], s, side(d)).start()

    base = jnp.concatenate([jnp.concatenate([meta[q]] * 16, axis=0).T[:block] for q in range(n_tp)], axis=0)
    lane = lax.broadcasted_iota(jnp.int32, (rows, 128), 1)
    earlier = lax.broadcasted_iota(jnp.int32, (rows, rows), 1) < lax.broadcasted_iota(jnp.int32, (rows, rows), 0)
    earlier = jnp.where(earlier, 1.0, 0.0).astype(bf)
    taken = jnp.zeros((1, 128), f32)
    places = base
    for k in range(2):
        named = jnp.where(lane.astype(f32) == base[:, k : k + 1], 1.0, 0.0)
        before = jnp.dot(earlier, named.astype(bf), preferred_element_type=f32) + taken
        rank = jnp.sum(before * named, axis=1, keepdims=True)
        taken = taken + jnp.sum(named, axis=0, keepdims=True)
        places = jnp.where(lane == k, base[:, k : k + 1] * cap + rank, places)
    slots_col[...] = places
    slots_row[...] = places.T[:8]

    width = heads.shape[1]

    def project(x, q):
        return jnp.dot(x, oc[pl.ds(pl.multiple_of(q * width, width), width)], preferred_element_type=f32)

    stream[...] = project(heads[...], t)
    for k, d in enumerate((-1, 1)):
        arrived(hall.at[side(d)], asem.at[k])
        ref = hall.at[side(d), pl.ds(k * half, half)]
        remote(ref, ref, sent.at[7], a2sem.at[k], s, side(-d)).start()
    stream[...] += project(hall[side(-1)], side(-1)) + project(hall[side(1)], side(1))
    for k in range(2):
        arrived(hall.at[side(2), pl.ds(k * half, half)], a2sem.at[k])
    for q in range(n_tp):
        ref = stream_in.at[pl.ds(q * block, block)]
        at_home = (t == q) & low

        @pl.when(at_home)
        def _():
            pltpu.make_async_copy(rows_in.at[:, pl.ds(q * feats, feats)], ref, local_sem.at[3]).wait()

        @pl.when(jnp.logical_not(at_home))
        def _():
            arrived(ref, ssem.at[q])

    total = stream[...] + project(hall[side(2)], side(2)) + stream_in[...].astype(f32)
    stream[...] = total

    part = jnp.sum(total * total, axis=1, keepdims=True)
    ssq[t] = jnp.broadcast_to(part, (rows, 128)).T[:8]
    for d in range(1, n_tp):
        remote(ssq.at[t], ssq.at[t], sent.at[8], qsem.at[d], s, side(d)).start()
    for d in range(1, n_tp):
        arrived(ssq.at[side(-d)], qsem.at[d])
    sums = ssq[0]
    for q in range(1, n_tp):
        sums = sums + ssq[q]
    inv = lax.rsqrt(sums / (feats * n_tp) + EPS)
    inv = jnp.concatenate([inv] * 16, axis=0).T[:, :1]
    normed = (stream[...] * inv * gain[:, pl.ds(pl.multiple_of(t * feats, feats), feats)]).astype(bf)

    own = pltpu.make_async_copy(send.at[s], xbuf.at[t, s], local_sem.at[0])

    def pack(j):
        plane = to_plane(j)
        place = plane * (group * cap) + lax.broadcasted_iota(jnp.int32, (group * cap, rows), 0)
        place = place.astype(f32)
        chosen = (place == slots_row[0:1, :]) | (place == slots_row[1:2, :])
        picked = jnp.dot(jnp.where(chosen, 1.0, 0.0).astype(bf), normed, preferred_element_type=f32)
        send[pl.ds(pl.multiple_of(plane * group, group), group)] = picked.astype(bf).reshape(group, cap, feats)
        return plane

    pack(0)
    own.start()

    def near(i, c):
        dest = z * group + lax.rem(w + i, group)
        remote(send.at[dest], xbuf.at[t, s], sent.at[0], dsem.at[0], dest, t).start()
        return c

    lax.fori_loop(1, group, near, 0)

    def far(j, c):
        plane = pack(j)

        def one(i, c):
            dest = plane * group + lax.rem(w + i, group)
            remote(send.at[dest], xbuf.at[t, s], sent.at[0], dsem.at[j], dest, t).start()
            return c

        return lax.fori_loop(0, group, one, c)

    lax.fori_loop(1, n_z, far, 0)
    for load in loads:
        load.wait()

    def chunk(q, j):
        return xbuf.at[q, pl.ds(from_plane(j) * group, group)]

    def stage_x(j):
        @pl.when(j == 0)
        def _():
            own.wait()
            arrived(xbuf.at[t, pl.ds(0, group - 1)], dsem.at[0])

        @pl.when(j > 0)
        def _():
            arrived(chunk(t, j), dsem.at[j])

        for k, d in enumerate((1, -1)):
            remote(chunk(t, j), chunk(t, j), sent.at[1], xsem.at[k, j], s, side(d)).start()

    def stage_x2(j):
        arrived(chunk(side(-1), j), xsem.at[0, j])
        arrived(chunk(side(1), j), xsem.at[1, j])
        d = 1 - 2 * lax.rem(j, 2)
        ref = chunk(side(-d), j)
        remote(ref, ref, sent.at[2], x2sem.at[j], s, side(d)).start()

    def stage_up(j):
        arrived(chunk(side(2), j), x2sem.at[j])
        first = pl.multiple_of(from_plane(j) * group, group)
        gate = jnp.zeros((group * cap, units), f32)
        upper = jnp.zeros((group * cap, units), f32)
        for q in range(n_tp):
            x = xbuf[q, pl.ds(first, group)].reshape(group * cap, feats)
            gate = gate + jnp.dot(x, gate_w[q * feats : (q + 1) * feats], preferred_element_type=f32)
            upper = upper + jnp.dot(x, up_w[q * feats : (q + 1) * feats], preferred_element_type=f32)
        act = gate / (1.0 + jnp.exp(-gate)) * upper
        plane = from_plane(j)
        hbuf[t, plane] = act.astype(bf)
        for k, d in enumerate((1, -1)):
            ref = hbuf.at[t, plane]
            remote(ref, ref, sent.at[3], hsem.at[k, j], s, side(d)).start()

    def stage_h2(j):
        plane = from_plane(j)
        arrived(hbuf.at[side(-1), plane], hsem.at[0, j])
        arrived(hbuf.at[side(1), plane], hsem.at[1, j])
        d = 1 - 2 * lax.rem(j, 2)
        ref = hbuf.at[side(-d), plane]
        remote(ref, ref, sent.at[4], h2sem.at[j], s, side(d)).start()

    def stage_down(j):
        plane = from_plane(j)
        arrived(hbuf.at[side(2), plane], h2sem.at[j])
        res = jnp.zeros((group * cap, feats), f32)
        for q in range(n_tp):
            res = res + jnp.dot(hbuf[q, plane], down_w[q * units : (q + 1) * units], preferred_element_type=f32)
        first = pl.multiple_of(plane * group, group)
        rbuf[pl.ds(first, group)] = res.astype(bf).reshape(group, cap, feats)

        @pl.when(j == 0)
        def _():
            pltpu.make_async_copy(rbuf.at[s], back.at[s], local_sem.at[1]).start()

            def one(i, c):
                dest = z * group + lax.rem(w + i, group)
                remote(rbuf.at[dest], back.at[s], sent.at[5], bsem.at[0], dest, t).start()
                return c

            lax.fori_loop(1, group, one, 0)

        @pl.when(j > 0)
        def _():
            def one(i, c):
                dest = plane * group + lax.rem(w + i, group)
                remote(rbuf.at[dest], back.at[s], sent.at[5], bsem.at[j], dest, t).start()
                return c

            lax.fori_loop(0, group, one, 0)

    stages = (stage_x, stage_x2, stage_up, stage_h2, stage_down)

    def step(i, c):
        for lag, stage in enumerate(stages):
            j = i - lag

            @pl.when((j >= 0) & (j < n_z))
            def _():
                stage(j)

        return c

    lax.fori_loop(0, n_z + len(stages) - 1, step, 0)

    pltpu.make_async_copy(rbuf.at[s], back.at[s], local_sem.at[1]).wait()
    arrived(back.at[pl.ds(0, group - 1)], bsem.at[0])

    def home(j, c):
        arrived(back.at[pl.ds(to_plane(j) * group, group)], bsem.at[j])
        return c

    lax.fori_loop(1, n_z, home, 0)

    table = back[...].reshape(n_sp * cap, feats)
    total = stream[...]
    place = lax.broadcasted_iota(jnp.int32, (rows, n_sp * cap), 1).astype(f32)
    for k in range(2):
        chosen = jnp.where(place == slots_col[:, k : k + 1], 1.0, 0.0).astype(bf)
        total = total + slots_col[:, 2 + k : 3 + k] * jnp.dot(chosen, table, preferred_element_type=f32)
    mix[...] = total.astype(bf)
    columns = out.at[:, pl.ds(pl.multiple_of(t * feats, feats), feats)]
    for b in range(n_tp):
        piece = mix.at[pl.ds(b * block, block)]
        if b < n_tp // 2:

            @pl.when(t == b)
            def _():
                pltpu.make_async_copy(piece, columns, local_sem.at[2]).start()

            @pl.when(t != b)
            def _():
                remote(piece, columns, sent.at[9], fsem.at[t], s, b).start()
        else:
            remote(piece, columns, sent.at[9], fsem.at[t], far_s, b).start()
    for q in range(n_tp):
        ref = out.at[:, pl.ds(q * feats, feats)]
        mine = (t == q) & low

        @pl.when(mine)
        def _():
            pltpu.make_async_copy(mix.at[pl.ds(0, block)], ref, local_sem.at[2]).wait()

        @pl.when(jnp.logical_not(mine))
        def _():
            arrived(ref, fsem.at[q])

    left(send.at[pl.ds(0, n_sp - 1)], sent.at[0])
    left(xbuf.at[pl.ds(0, 2)], sent.at[1])
    left(xbuf.at[0], sent.at[2])
    left(hbuf.at[pl.ds(0, 2)], sent.at[3])
    left(hbuf.at[0], sent.at[4])
    left(rbuf.at[pl.ds(0, n_sp - 1)], sent.at[5])
    left(hall.at[pl.ds(0, 2)], sent.at[6])
    left(hall.at[0], sent.at[7])
    left(ssq.at[pl.ds(0, n_tp - 1)], sent.at[8])

    @pl.when(low)
    def _():
        left(mix.at[pl.ds(0, (n_tp - 1) * block)], sent.at[9])
        left(mix.at[pl.ds(0, (n_tp - 1) * block)], sent.at[10])

    @pl.when(jnp.logical_not(low))
    def _():
        left(mix, sent.at[9])
        left(mix, sent.at[10])


def send_stream(n_sp, n_tp, rows_in, stream_in, sent, local_sem, ssem):
    s, t = lax.axis_index("sp"), lax.axis_index("tp")
    far_s, low = n_sp - 1 - s, t < n_tp // 2
    block, feats = rows_in.shape[0], stream_in.shape[1]
    sp_home = jnp.where(low, s, far_s)
    slab = stream_in.at[pl.ds(pl.multiple_of(t * block, block), block)]
    for q in range(n_tp):
        piece = rows_in.at[:, pl.ds(q * feats, feats)]
        at_home = (t == q) & low

        @pl.when(at_home)
        def _():
            pltpu.make_async_copy(piece, slab, local_sem.at[3]).start()

        @pl.when(jnp.logical_not(at_home))
        def _():
            pltpu.make_async_remote_copy(
                src_ref=piece, dst_ref=slab, send_sem=sent.at[10], recv_sem=ssem.at[t], device_id=(sp_home, q),
                device_id_type=MESH).start()


def layer_kernel(dims, queries_one, queries_two, keys_one, keys_two, values, meta_in, out_w, down_w, lam, head_gain,
                 rows_in, norm_gain, gate_h, up_h, out, heads, meta, oc, down, *rest):
    n_z, n_y, n_c, n_tp, _ = dims
    stream_in, hall, slots_row, slots_col, gate_w, up_w, *tail = rest[N_FRONT:]
    late = functools.partial(
        send_stream, n_z * n_y * n_c, n_tp, rows_in, stream_in, tail[8], tail[9], tail[-1])
    attention_part(
        dims, late, queries_one, queries_two, keys_one, keys_two, values, meta_in, out_w, down_w, lam, head_gain,
        heads, meta, oc, down, *rest[:N_FRONT],
    )
    experts_part(
        n_z * n_y * n_c, n_tp, n_y * n_c, heads, rows_in, norm_gain, meta, gate_h, up_h,
        out, stream_in, hall, slots_row, slots_col, oc, gate_w, up_w, down, *tail,
    )


def layer(queries_one, queries_two, keys_one, keys_two, values, meta, out_w, down_w, lam, head_gain,
          rows_in, norm_gain, gate_w, up_w, dims):
    n_z, n_y, n_c, n_tp, split = dims
    n_sp, group = n_z * n_y * n_c, n_y * n_c
    rows = queries_one.shape[0]
    feats = out_w.shape[1] // n_tp
    units, cap = gate_w.shape[1], CAP
    turn = n_z // 2
    bf, f32 = jnp.bfloat16, jnp.float32
    dma = pltpu.SemaphoreType.DMA
    vmem, hbm = pl.BlockSpec(memory_space=pltpu.VMEM), pl.BlockSpec(memory_space=pl.ANY)
    smem = pl.BlockSpec(memory_space=pltpu.SMEM)
    first = [
        pltpu.VMEM((n_z, n_y, n_c, rows, 2 * HEAD_DIM + VAL_DIM), bf),
        pltpu.VMEM((2, rows // 2, 2 * HEAD_DIM), bf),
        pltpu.VMEM((2, 2, rows, HEAD_DIM), bf),
        pltpu.VMEM((2, 2, rows, 128), f32),
        pltpu.VMEM((2, 2, rows, 128), f32),
        pltpu.VMEM((2, 2, rows, VAL_DIM), f32),
        dma((12,)), dma((7,)), dma((2,)), dma((n_tp,)), dma((n_tp,)), dma((n_tp,)),
        dma((2, turn + 1)), dma((n_z, 2)), dma((n_z,)), dma((2,)), dma((1,)), dma((4, 2, turn + 1)), dma((n_z,)),
    ]
    assert len(first) == N_FRONT
    second = [
        pltpu.VMEM((rows, feats), bf),
        pltpu.VMEM((n_tp, rows, 2 * VAL_DIM), bf),
        pltpu.VMEM((8, rows), f32),
        pltpu.VMEM((rows, 128), f32),
        pltpu.VMEM(gate_w.shape, bf),
        pltpu.VMEM(up_w.shape, bf),
        pltpu.VMEM((rows, feats), f32),
        pltpu.VMEM((n_tp, 8, rows), f32),
        pltpu.VMEM((n_sp, cap, feats), bf),
        pltpu.VMEM((n_tp, n_sp, cap, feats), bf),
        pltpu.VMEM((n_tp, n_z, group * cap, units), bf),
        pltpu.VMEM((n_sp, cap, feats), bf),
        pltpu.VMEM((n_sp, cap, feats), bf),
        pltpu.VMEM((rows, feats), bf),
        dma((11,)), dma((4,)), dma((4,)), dma((2,)), dma((2,)), dma((n_tp,)), dma((n_z,)), dma((2, n_z)),
        dma((n_z,)), dma((2, n_z)), dma((n_z,)), dma((n_z,)), dma((n_tp,)), dma((n_tp,)),
    ]
    return pl.pallas_call(
        functools.partial(layer_kernel, dims),
        out_shape=jax.ShapeDtypeStruct((rows // n_tp, feats * n_tp), bf),
        in_specs=[vmem, vmem, hbm, hbm, hbm, vmem, hbm, hbm, smem, vmem, vmem, vmem, hbm, hbm],
        out_specs=vmem,
        scratch_shapes=[
            pltpu.VMEM((rows, 2 * VAL_DIM), bf),
            pltpu.VMEM((n_tp,) + meta.shape, f32),
            pltpu.VMEM((n_tp * out_w.shape[0], feats), bf),
            pltpu.VMEM((n_tp * down_w.shape[0], feats), bf),
        ]
        + first
        + second,
        compiler_params=pltpu.CompilerParams(
            collective_id=0, has_side_effects=True, vmem_limit_bytes=60 * 1024 * 1024),
        name="layer",
    )(queries_one, queries_two, keys_one, keys_two, values, meta, out_w, down_w, lam, head_gain,
      rows_in, norm_gain, gate_w, up_w)


def shards(
    stream_in, queries_one, queries_two, keys_one, keys_two, values, lambdas, head_gain, out_weight,
    norm_gain, expert_ids, route_weight, gate_weight, up_weight, down_weight,
):
    meta = jnp.concatenate([expert_ids.astype(jnp.float32), route_weight], 1).T
    meta = jnp.pad(meta, ((0, 8 - meta.shape[0]), (0, 128 - meta.shape[1])))
    return layer(
        queries_one, queries_two, keys_one, keys_two, values, meta, out_weight, down_weight[0], lambdas, head_gain[None],
        stream_in, norm_gain[None], gate_weight[0], up_weight[0], CHIPS + (lax.axis_size("tp"), SPLIT),
    )


def solution(mesh):
    return jax.shard_map(
        shards,
        mesh=mesh,
        in_specs=(
            P(("sp", "tp"), None),
            P("sp", "tp"),
            P("sp", "tp"),
            P("sp", "tp"),
            P("sp", "tp"),
            P("sp", "tp"),
            P("tp"),
            P(),
            P("tp", None),
            P(),
            P(("sp", "tp"), None),
            P(("sp", "tp"), None),
            P("sp", None, "tp"),
            P("sp", None, "tp"),
            P("sp", "tp", None),
        ),
        out_specs=P(("sp", "tp"), None),
        check_vma=False,
    )
```
